256 devices in a mesh: sp: 32 (over z, y), tp: 8 (over x, core).
Axes of the slice: x: 4, y: 4, z: 8, core: 2. Of those that a mesh axis runs over, the one named last changes fastest.
Arguments:
- latent: bfloat16 [16384, 4096], P(('sp', 'tp')), may hold values from -3 to 3
- context: bfloat16 [1024, 4096], P('sp'), may hold values from -6 to 6
- cond: float32 [4096], replicated, may hold values from -6 to 6
- ctx_cond: float32 [4096], replicated, may hold values from -6 to 6
- w_shift: bfloat16 [4096, 4096], P('sp', 'tp'), may hold values from -0.1875 to 0.1875
- w_scale: bfloat16 [4096, 4096], P('sp', 'tp'), may hold values from -0.09375 to 0.15478516
- w_gate: bfloat16 [4096, 4096], P('sp', 'tp'), may hold values from -0.1875 to 0.1875
- w_query: bfloat16 [4096, 2048], P(None, 'tp'), may hold values from -0.09375 to 0.09375
- key_weight: bfloat16 [4096, 1024], P(None, 'tp'), may hold values from -0.09375 to 0.09375
- value_weight: bfloat16 [4096, 1024], P(None, 'tp'), may hold values from -0.09375 to 0.09375
- w_out: bfloat16 [2048, 4096], P('tp'), may hold values from -0.125 to 0.125
- sink: float32 [16], replicated, may hold values from 4 to 8
Outputs:
- mixed: bfloat16 [16384, 4096], P(('sp', 'tp'))
The draws below stay inside these ranges and needn't reach their ends.
All inputs are finite; a program needn't handle non-finite values.
Results may differ from the reference program's by a relative error of at most 0.035.
Values may be sent and summed in bfloat16 or wider, within the bound.
A program may use at most 64 MiB of HBM per device.

```python
import math
import jax
import jax.numpy as jnp
from jax import lax

MODEL_WIDTH = 4096
HEAD_SIZE = 128
QUERY_HEADS = 16
KEY_VALUE_HEADS = 8
WINDOW_SIDE = 128
GRID_WIDTH = 64
CONTEXT_TOKENS = 1024
LATENT_TOKENS = 16384
N_TP = 8


def draw_w_scale(key, part):
    first, second = jax.random.split(jax.random.fold_in(key, 11))
    spread = 2.0 / math.sqrt(MODEL_WIDTH)
    values = jnp.clip(jax.random.normal(first, (MODEL_WIDTH, MODEL_WIDTH), jnp.float32) * spread, -3.0 * spread, 3.0 * spread)
    return values.astype(jnp.bfloat16)


def level_of(stream_key, dims, cuts, least, largest):
    loudness, own = 1.0, jax.random.fold_in(stream_key, 6)
    for dim, shards_of in cuts:
        draws = jnp.exp(jax.random.uniform(jax.random.fold_in(own, dim), (shards_of,), jnp.float32, least / len(cuts), largest / len(cuts)))
        loudness = loudness * jnp.repeat(draws, dims[dim] // shards_of).reshape([-1 if axis == dim else 1 for axis in range(len(dims))])
    return loudness


def normal_values(stream_key, dims, scale, most, shards=(), kind=jnp.bfloat16):
    level = level_of(stream_key, dims, shards, -0.22, 0.18) if shards else 1.0
    values = jax.random.normal(stream_key, dims, jnp.float32) * scale * level
    return jnp.minimum(jnp.maximum(values, -most), most).astype(kind)


def setup_inputs(seed: int = 0) -> dict:
    splits = jax.random.split(jax.random.key(seed), 13)
    return {
        "latent": normal_values(splits[0], (LATENT_TOKENS, MODEL_WIDTH), 0.5, 3.0, ((0, 256),)),
        "context": normal_values(splits[1], (CONTEXT_TOKENS, MODEL_WIDTH), 1.0, 6.0, ((0, 32),)),
        "cond": normal_values(splits[2], (MODEL_WIDTH,), 1.0, 6.0, (), jnp.float32),
        "ctx_cond": normal_values(splits[3], (MODEL_WIDTH,), 1.0, 6.0, (), jnp.float32),
        "w_shift": normal_values(splits[4], (MODEL_WIDTH, MODEL_WIDTH), (MODEL_WIDTH // 4) ** -0.5, 0.1875, ((0, 32), (1, 8))),
        "w_scale": draw_w_scale(jax.random.fold_in(splits[12], 71), 0),
        "w_gate": normal_values(splits[6], (MODEL_WIDTH, MODEL_WIDTH), (MODEL_WIDTH // 4) ** -0.5, 0.1875, ((0, 32), (1, 8))),
        "w_query": normal_values(splits[7], (MODEL_WIDTH, QUERY_HEADS * HEAD_SIZE), MODEL_WIDTH ** -0.5, 0.09375, ((1, 8),)),
        "key_weight": normal_values(splits[8], (MODEL_WIDTH, KEY_VALUE_HEADS * HEAD_SIZE), MODEL_WIDTH ** -0.5, 0.09375, ((1, 8),)),
        "value_weight": normal_values(splits[9], (MODEL_WIDTH, KEY_VALUE_HEADS * HEAD_SIZE), MODEL_WIDTH ** -0.5, 0.09375, ((1, 8),)),
        "w_out": normal_values(splits[10], (QUERY_HEADS * HEAD_SIZE, MODEL_WIDTH), (QUERY_HEADS * HEAD_SIZE) ** -0.5, 0.125, ((0, 8),)),
        "sink": jnp.clip(jax.random.uniform(splits[11], (QUERY_HEADS,), jnp.float32, 4.0, 8.0), 4.0, 8.0),
    }


EPS = 1e-05
THETA = 10000.0
MASKED = -1e+30

def layer_norm(rows):
    values = rows.astype(jnp.float32)
    mean = lax.optimization_barrier(jnp.mean(values, axis=-1, keepdims=True))
    var = lax.optimization_barrier(jnp.mean(jnp.square(values - mean), axis=-1, keepdims=True))
    return (values - mean) * lax.rsqrt(var + EPS)

def rotate_half(values, token_position, width):
    half = width // 2
    inverse = THETA ** (-jnp.arange(half, dtype=jnp.float32) * 2.0 / width)
    angle = token_position.astype(jnp.float32)[:, None] * inverse[None, :]
    cosine = jnp.cos(angle)[:, None, :]
    sine = jnp.sin(angle)[:, None, :]
    first = values[..., :half]
    second = values[..., half:]
    return jnp.concatenate([first * cosine - second * sine, second * cosine + first * sine], axis=-1)

def axial_rotation(heads, token_position, grid):
    width = heads.shape[-1] // 2
    values = heads.astype(jnp.float32)
    turned = jnp.concatenate([rotate_half(values[..., :width], token_position // grid, width), rotate_half(values[..., width:], token_position % grid, width)], axis=-1)
    return turned.astype(jnp.bfloat16)

def sink_weights(scores, sink_column):
    top = jnp.maximum(lax.optimization_barrier(jnp.max(scores, axis=-1, keepdims=True)), sink_column)
    expo = jnp.exp(scores - top)
    return (expo / (lax.optimization_barrier(jnp.sum(expo, axis=-1, keepdims=True)) + jnp.exp(sink_column - top))).astype(jnp.bfloat16)

def reference(latent, context, cond, ctx_cond, w_shift, w_scale, w_gate, w_query, key_weight, value_weight, w_out, sink):
    act = jax.nn.silu(jnp.stack([cond, ctx_cond])).astype(jnp.bfloat16)
    shift = jnp.dot(act, w_shift, preferred_element_type=jnp.float32)
    scale = jnp.dot(act, w_scale, preferred_element_type=jnp.float32)
    gate = jnp.dot(act[0:1], w_gate, preferred_element_type=jnp.float32)[0]
    latent_mod = (layer_norm(latent) * (1.0 + scale[0]) + shift[0]).astype(jnp.bfloat16)
    ctx_mod = (layer_norm(context) * (1.0 + scale[1]) + shift[1]).astype(jnp.bfloat16)
    query_group = QUERY_HEADS // KEY_VALUE_HEADS
    query = jnp.dot(latent_mod, w_query, preferred_element_type=jnp.float32).astype(jnp.bfloat16)
    key = jnp.dot(latent_mod, key_weight, preferred_element_type=jnp.float32).astype(jnp.bfloat16)
    value_rows = jnp.dot(latent_mod, value_weight, preferred_element_type=jnp.float32).astype(jnp.bfloat16)
    context_key_rows = jnp.dot(ctx_mod, key_weight, preferred_element_type=jnp.float32).astype(jnp.bfloat16)
    context_value_rows = jnp.dot(ctx_mod, value_weight, preferred_element_type=jnp.float32).astype(jnp.bfloat16)
    token_position = jnp.arange(LATENT_TOKENS, dtype=jnp.int32)
    rotated_query = axial_rotation(query.reshape(LATENT_TOKENS, QUERY_HEADS, HEAD_SIZE), token_position, GRID_WIDTH)
    rotated_key = axial_rotation(key.reshape(LATENT_TOKENS, KEY_VALUE_HEADS, HEAD_SIZE), token_position, GRID_WIDTH)
    padded_key = jnp.pad(rotated_key, ((WINDOW_SIDE, WINDOW_SIDE), (0, 0), (0, 0)))
    value_padded_rows = jnp.pad(value_rows.reshape(LATENT_TOKENS, KEY_VALUE_HEADS, HEAD_SIZE), ((WINDOW_SIDE, WINDOW_SIDE), (0, 0), (0, 0)))
    context_key_wide = context_key_rows.reshape(CONTEXT_TOKENS, KEY_VALUE_HEADS, HEAD_SIZE).astype(jnp.float32)
    context_value_wide = context_value_rows.reshape(CONTEXT_TOKENS, KEY_VALUE_HEADS, HEAD_SIZE).astype(jnp.float32)
    sink_column = sink.reshape(KEY_VALUE_HEADS, query_group)[:, :, None, None]
    factor = HEAD_SIZE ** (-0.5)
    block_list = LATENT_TOKENS // WINDOW_SIDE
    query_block_list = rotated_query.reshape(block_list, WINDOW_SIDE, KEY_VALUE_HEADS, query_group, HEAD_SIZE)

    def one_block(item):
        qblk, index = item
        start = (index * WINDOW_SIDE).astype(jnp.int32)
        kblk = lax.dynamic_slice_in_dim(padded_key, start, 3 * WINDOW_SIDE, 0).astype(jnp.float32)
        vblk = lax.dynamic_slice_in_dim(value_padded_rows, start, 3 * WINDOW_SIDE, 0).astype(jnp.float32)
        q32 = qblk.astype(jnp.float32)
        band_scores = jnp.einsum('qhgd,khd->hgqk', q32, kblk) * factor
        qpos = start + jnp.arange(WINDOW_SIDE, dtype=jnp.int32)
        kpos = start - WINDOW_SIDE + jnp.arange(3 * WINDOW_SIDE, dtype=jnp.int32)
        valid = (jnp.abs(kpos[None, :] - qpos[:, None]) <= WINDOW_SIDE) & (kpos[None, :] >= 0) & (kpos[None, :] < LATENT_TOKENS)
        band_scores = jnp.where(valid[None, None], band_scores, MASKED)
        ctx_scores = jnp.einsum('qhgd,khd->hgqk', q32, context_key_wide) * factor
        weights = sink_weights(jnp.concatenate([band_scores, ctx_scores], axis=-1), sink_column).astype(jnp.float32)
        out = jnp.einsum('hgqk,khd->qhgd', weights[..., :3 * WINDOW_SIDE], vblk) + jnp.einsum('hgqk,khd->qhgd', weights[..., 3 * WINDOW_SIDE:], context_value_wide)
        return out.astype(jnp.bfloat16).reshape(WINDOW_SIDE, QUERY_HEADS * HEAD_SIZE)
    attended = lax.map(one_block, (query_block_list, jnp.arange(block_list, dtype=jnp.int32))).reshape(LATENT_TOKENS, QUERY_HEADS * HEAD_SIZE)
    columns = QUERY_HEADS * HEAD_SIZE // N_TP
    projected = jnp.zeros((LATENT_TOKENS, MODEL_WIDTH), jnp.float32)
    for group_index in range(N_TP):
        lower = group_index * columns
        partial_product = jnp.dot(attended[:, lower:lower + columns], w_out[lower:lower + columns], preferred_element_type=jnp.float32).astype(jnp.bfloat16)
        projected = projected + partial_product.astype(jnp.float32)
    return (latent.astype(jnp.float32) + gate[None, :] * projected).astype(jnp.bfloat16)
```

```python
import jax
import jax.numpy as jnp
import numpy as np
from jax import lax
from jax.experimental import pallas as pl
from jax.experimental.pallas import tpu as pltpu
from jax.sharding import PartitionSpec as P

MESH = pl.DeviceIdType.MESH
F32 = jnp.float32
BF16 = jnp.bfloat16

NX, NY, NZ, NT = 4, 4, 8, 8
NSP = NY * NZ
HEAD = 128
SIDE = 128
BLOCK = 64
WIDTH = 4096
HALF = WIDTH // 2
PAIR = 2 * BLOCK
TOKENS = 16384
CTX_ROWS = 32
EPS = 1e-05
THETA = 10000.0
MASKED = -1e30
PIECES = 4
PIECE = HALF // PIECES


def kernel(
    latent, context, cond, ctx_cond, w_shift, w_scale, w_gate, wq, wk, wv, wo, sink, inverse, out,
    x_raw, x_mod, w_all, w_out, w_modulation, ctx_raw, ctx_mod, y_buf, z_buf, t_buf, mod_rows,
    product, query, kv, ckv, attended, partial, from_left, from_right, left_done, right_done,
    l_sem, ag_s, ag_r, w_s, w_r, y_s, y_r, z_s, z_r, t_s, t_r, cz_s, cz_r, cy_s, cy_r, cc_s, cc_r,
    kv_s, kv_r, h_s, h_r, o_s, o_r, d_s, d_r, c_s, c_r,
):
    sp = lax.axis_index("sp")
    tp = lax.axis_index("tp")
    z, y = sp // NY, sp % NY
    x, core = tp // 2, tp % 2
    sibling = x * 2 + 1 - core
    right, opposite, left = (x + 1) % NX, (x + 2) % NX, (x + 3) % NX
    sp_next, sp_back = (sp + 1) % NSP, (sp + NSP - 1) % NSP
    to_right, to_left = (sp, right * 2 + core), (sp, left * 2 + core)
    to_sibling = (sp, sibling)

    def remote(src, dst, send, recv, device):
        return pltpu.make_async_remote_copy(
            src_ref=src, dst_ref=dst, send_sem=send, recv_sem=recv, device_id=device, device_id_type=MESH
        )

    sent = []

    def send(*args):
        copy = remote(*args)
        copy.start()
        sent.append(copy)

    def received(dst, send_sem, recv_sem):
        remote(dst, dst, send_sem, recv_sem, to_sibling).wait_recv()

    local = [
        pltpu.make_async_copy(w_shift, w_modulation.at[0], l_sem.at[0]),
        pltpu.make_async_copy(w_scale, w_modulation.at[1], l_sem.at[1]),
        pltpu.make_async_copy(w_gate, w_modulation.at[2], l_sem.at[2]),
        pltpu.make_async_copy(latent, x_raw.at[x], l_sem.at[3]),
        pltpu.make_async_copy(context, ctx_raw, l_sem.at[4]),
        pltpu.make_async_copy(wq, w_all.at[core, :, 0:256], l_sem.at[5]),
        pltpu.make_async_copy(wk, w_all.at[core, :, 256:384], l_sem.at[6]),
        pltpu.make_async_copy(wv, w_all.at[core, :, 384:512], l_sem.at[7]),
        pltpu.make_async_copy(wo, w_out.at[core], l_sem.at[8]),
    ]
    for copy in local:
        copy.start()

    barrier = pltpu.get_barrier_semaphore()
    greeted = [(sp, (tp + d) % NT) for d in range(1, NT)]
    greeted += [(z * NY + (y + d) % NY, tp) for d in range(1, NY)]
    greeted += [(((z + d) % NZ) * NY + y, tp) for d in range(1, NZ)]
    greeted += [(sp_next, tp), (sp_next, sibling), (sp_back, tp), (sp_back, sibling)]
    for device in greeted:
        pl.semaphore_signal(barrier, inc=1, device_id=device, device_id_type=MESH)

    act = jnp.concatenate(
        [jax.nn.silu(cond[pl.ds(sp, 1), :]), jax.nn.silu(ctx_cond[pl.ds(sp, 1), :]), jnp.zeros((6, 128), F32)],
        axis=0,
    ).astype(BF16)
    y_buf[y] = jnp.zeros((24, 128), F32)
    for i in range(3):
        local[i].wait()
        part = jnp.dot(act, w_modulation[i], preferred_element_type=F32)
        for row in range(2 if i < 2 else 1):
            for c in range(4):
                at = (2 * i + row) * 4 + c
                y_buf[y, at : at + 1, :] = part[row : row + 1, c * 128 : (c + 1) * 128]

    pl.semaphore_wait(barrier, len(greeted))

    for d in range(1, NY):
        send(y_buf.at[y], y_buf.at[y], y_s.at[d - 1], y_r.at[d - 1], (z * NY + (y + d) % NY, tp))

    local[3].wait()
    first, second = pl.ds(0, BLOCK // 2), pl.ds(BLOCK // 2, BLOCK // 2)

    def gather(block, rows, i, device):
        send(x_raw.at[block, rows, :], x_raw.at[block, rows, :], ag_s.at[i], ag_r.at[i], device)

    gather(x, first, 0, to_right)
    gather(x, second, 1, to_left)
    gather(x, second, 2, to_right)
    gather(x, first, 3, to_left)

    send(wq, w_all.at[core, :, 0:256], w_s.at[0], w_r.at[0], to_sibling)
    send(wk, w_all.at[core, :, 256:384], w_s.at[1], w_r.at[1], to_sibling)
    send(wv, w_all.at[core, :, 384:512], w_s.at[2], w_r.at[2], to_sibling)
    send(wo, w_out.at[core], w_s.at[3], w_r.at[3], to_sibling)

    for d in range(1, NY):
        received(y_buf.at[(y + NY - d) % NY], y_s.at[d - 1], y_r.at[d - 1])
    z_buf[z] = jnp.sum(y_buf[...], axis=0)
    for d in (4, 3, 5, 2, 6, 1, 7):
        send(z_buf.at[z], z_buf.at[z], z_s.at[d - 1], z_r.at[d - 1], (((z + d) % NZ) * NY + y, tp))
    for d in range(1, NZ):
        received(z_buf.at[(z + NZ - d) % NZ], z_s.at[d - 1], z_r.at[d - 1])
    t_buf[tp] = jnp.sum(z_buf[...], axis=0)
    for d in range(1, NT):
        send(t_buf.at[tp], t_buf.at[tp], t_s.at[d - 1], t_r.at[d - 1], (sp, (tp + d) % NT))

    received(x_raw.at[left, first, :], ag_s.at[0], ag_r.at[0])
    gather(left, first, 4, to_right)
    received(x_raw.at[right, second, :], ag_s.at[1], ag_r.at[1])
    gather(right, second, 5, to_left)

    for d in range(1, NT):
        received(t_buf.at[(tp + NT - d) % NT], t_s.at[d - 1], t_r.at[d - 1])
    for t in range(NT):
        for row in range(5):
            for c in range(4):
                at = t * 512 + c * 128
                value = t_buf[t, row * 4 + c : row * 4 + c + 1, :]
                mod_rows[row : row + 1, at : at + 128] = 1.0 + value if row in (2, 3) else value

    def modulate(read, write, which):
        rows = read()
        values = rows.astype(F32)
        mean = jnp.mean(values, axis=-1, keepdims=True)
        centred = values - mean
        var = jnp.mean(jnp.square(centred), axis=-1, keepdims=True)
        normal = centred * lax.rsqrt(var + EPS)
        write((normal * mod_rows[2 + which : 3 + which, :] + mod_rows[which : which + 1, :]).astype(BF16))

    local[4].wait()

    @pl.loop(0, CTX_ROWS // 16)
    def _(i):
        at = pl.ds(pl.multiple_of(i * 16, 16), 16)

        def write(value):
            ctx_mod[at, :] = value

        modulate(lambda: ctx_raw[at, :], write, 1)

    for copy in local[5:9]:
        copy.wait()
    ckv[core, y, z] = jnp.dot(ctx_mod[...], w_all[core, :, 256:512], preferred_element_type=F32).astype(BF16)
    own = ckv.at[core, y, z]
    for d in (4, 3, 5, 2, 6, 1, 7):
        send(own, own, cz_s.at[d - 1], cz_r.at[d - 1], (((z + d) % NZ) * NY + y, tp))

    received(x_raw.at[left, second, :], ag_s.at[2], ag_r.at[2])
    received(x_raw.at[right, first, :], ag_s.at[3], ag_r.at[3])
    received(x_raw.at[opposite, first, :], ag_s.at[4], ag_r.at[4])
    received(x_raw.at[opposite, second, :], ag_s.at[5], ag_r.at[5])

    @pl.loop(0, NX * BLOCK // 16)
    def _(i):
        block = i // (BLOCK // 16)
        at = pl.ds(pl.multiple_of((i % (BLOCK // 16)) * 16, 16), 16)

        def write(value):
            x_mod[pl.ds(pl.multiple_of(i * 16, 16), 16), :] = value

        modulate(lambda: x_raw[block, at, :], write, 0)

    for d in range(1, NZ):
        received(ckv.at[core, y, (z + NZ - d) % NZ], cz_s.at[d - 1], cz_r.at[d - 1])
    line = ckv.at[core, y]
    for d in (2, 1, 3):
        send(line, line, cy_s.at[d - 1], cy_r.at[d - 1], (z * NY + (y + d) % NY, tp))
    send(line, line, cc_s.at[0], cc_r.at[0], to_sibling)

    other = w_all.at[1 - core]
    received(other.at[:, 0:256], w_s.at[0], w_r.at[0])
    received(other.at[:, 256:384], w_s.at[1], w_r.at[1])
    received(other.at[:, 384:512], w_s.at[2], w_r.at[2])

    @pl.loop(0, 2)
    def _(j):
        for c in range(2):
            product[j, c] = jnp.dot(
                x_mod[...], w_all[j, :, c * 256 : (c + 1) * 256], preferred_element_type=F32
            ).astype(BF16)

    lane = lax.broadcasted_iota(jnp.int32, (BLOCK, HEAD), 1)
    column = lax.broadcasted_iota(jnp.int32, (BLOCK, HEAD), 0)
    by_row = lane < HEAD // 2
    is_first = lane % (HEAD // 2) < HEAD // 4

    @pl.loop(0, NX)
    def _(b):
        grid_row = sp * NT + b * 2 + core
        position = jnp.where(by_row, grid_row, column).astype(F32)
        angle = position * inverse[0:1, :]
        cosine = jnp.cos(angle)
        sine = jnp.sin(angle)
        sine = jnp.where(is_first, -sine, sine)

        def turned(value):
            value = value.astype(F32)
            partner = jnp.where(is_first, pltpu.roll(value, 96, 1), pltpu.roll(value, 32, 1))
            return (value * cosine + partner * sine).astype(BF16)

        rows = pl.ds(pl.multiple_of(b * BLOCK, BLOCK), BLOCK)
        for j in range(2):
            for g in range(2):
                query[b, 2 * j + g] = turned(product[j, 0, rows, g * HEAD : (g + 1) * HEAD])
            kv[b + 1, core, :, j * HEAD : (j + 1) * HEAD] = turned(product[j, 1, rows, 0:HEAD])
            kv[b + 1, core, :, (2 + j) * HEAD : (3 + j) * HEAD] = product[j, 1, rows, HEAD : 2 * HEAD]

    for k, tp_there in enumerate((tp, sibling)):
        send(kv.at[NX, core], kv.at[0, core], h_s.at[k], h_r.at[k], (sp_next, tp_there))
        send(kv.at[1, core], kv.at[NX + 1, core], h_s.at[2 + k], h_r.at[2 + k], (sp_back, tp_there))
    for b in range(NX):
        send(kv.at[b + 1, core], kv.at[b + 1, core], kv_s.at[b], kv_r.at[b], to_sibling)

    for d in range(1, NY):
        line = ckv.at[core, (y + NY - d) % NY]
        received(line, cy_s.at[d - 1], cy_r.at[d - 1])
        send(line, line, cc_s.at[d], cc_r.at[d], to_sibling)

    for k, core_there in enumerate((core, 1 - core)):
        received(kv.at[0, core_there], h_s.at[k], h_r.at[k])
        received(kv.at[NX + 1, core_there], h_s.at[2 + k], h_r.at[2 + k])
    for b in range(NX):
        received(kv.at[b + 1, 1 - core], kv_s.at[b], kv_r.at[b])
    for d in range(NY):
        received(ckv.at[1 - core, (y + NY - d) % NY], cc_s.at[d], cc_r.at[d])

    factor = HEAD ** (-0.5)
    i_query = lax.broadcasted_iota(jnp.int32, (PAIR, 3 * PAIR), 0) % BLOCK + core * BLOCK
    i_key = lax.broadcasted_iota(jnp.int32, (PAIR, 3 * PAIR), 1) - PAIR
    near = jnp.abs(i_key - i_query) <= SIDE
    upper = lax.broadcasted_iota(jnp.int32, (PAIR, 1), 0) < BLOCK
    across = (((1,), (1,)), ((), ()))

    @pl.loop(0, NX)
    def _(b):
        place = i_key + (sp * NT * BLOCK + b * PAIR)
        valid = near & (place >= 0) & (place < TOKENS)
        for h in range(2):
            q = query[b, 2 * h : 2 * h + 2].reshape(PAIR, HEAD)
            k_band = kv[pl.ds(b, 3), :, :, h * HEAD : (h + 1) * HEAD].reshape(3 * PAIR, HEAD)
            v_band = kv[pl.ds(b, 3), :, :, (2 + h) * HEAD : (3 + h) * HEAD].reshape(3 * PAIR, HEAD)
            k_ctx = ckv[h, :, :, :, 0:HEAD].reshape(NSP * CTX_ROWS, HEAD)
            v_ctx = ckv[h, :, :, :, HEAD : 2 * HEAD].reshape(NSP * CTX_ROWS, HEAD)
            s_band = lax.dot_general(q, k_band, across, preferred_element_type=F32) * factor
            s_band = jnp.where(valid, s_band, MASKED)
            s_ctx = lax.dot_general(q, k_ctx, across, preferred_element_type=F32) * factor
            sinks = jnp.where(upper, sink[4 * x + 2 * h], sink[4 * x + 2 * h + 1])
            top = jnp.maximum(
                jnp.maximum(jnp.max(s_band, axis=-1, keepdims=True), jnp.max(s_ctx, axis=-1, keepdims=True)), sinks
            )
            e_band = jnp.exp(s_band - top)
            e_ctx = jnp.exp(s_ctx - top)
            total = (
                jnp.sum(e_band, axis=-1, keepdims=True)
                + jnp.sum(e_ctx, axis=-1, keepdims=True)
                + jnp.exp(sinks - top)
            )
            value = jnp.dot(e_band.astype(BF16), v_band, preferred_element_type=F32)
            value += jnp.dot(e_ctx.astype(BF16), v_ctx, preferred_element_type=F32)
            value = (value / total).astype(BF16)
            rows = pl.ds(pl.multiple_of(b * BLOCK, BLOCK), BLOCK)
            for g in range(2):
                attended[rows, (2 * h + g) * HEAD : (2 * h + g + 1) * HEAD] = value[g * BLOCK : (g + 1) * BLOCK]

    received(w_out.at[1 - core], w_s.at[3], w_r.at[3])
    for c in range(PIECES):
        for half in range(2):
            at = half * HALF + c * PIECE
            columns = slice(at, at + PIECE)
            result = jnp.dot(attended[:, 0:256], w_out[0, :, columns], preferred_element_type=F32)
            result += jnp.dot(attended[:, 256:512], w_out[1, :, columns], preferred_element_type=F32)
            result = result.astype(BF16)
            for b in range(NX):
                partial[b, :, columns] = result[b * BLOCK : (b + 1) * BLOCK]
        lower = pl.ds(c * PIECE, PIECE)
        higher = pl.ds(HALF + c * PIECE, PIECE)
        send(partial.at[opposite, :, lower], from_left.at[:, lower], o_s.at[0, c], o_r.at[0, c], to_right)
        send(partial.at[opposite, :, higher], from_right.at[:, lower], o_s.at[1, c], o_r.at[1, c], to_left)
    low, high = pl.ds(0, HALF), pl.ds(HALF, HALF)
    send(partial.at[right, :, high], left_done.at[:, high], d_s.at[0], d_r.at[0], to_right)
    send(partial.at[left, :, low], right_done.at[:, low], d_s.at[1], d_r.at[1], to_left)
    for c in range(PIECES):
        lower = pl.ds(c * PIECE, PIECE)
        higher = pl.ds(HALF + c * PIECE, PIECE)
        received(from_left.at[:, lower], o_s.at[0, c], o_r.at[0, c])
        partial[right, :, lower] = (partial[right, :, lower].astype(F32) + from_left[:, lower].astype(F32)).astype(BF16)
        send(partial.at[right, :, lower], left_done.at[:, lower], c_s.at[0, c], c_r.at[0, c], to_right)
        received(from_right.at[:, lower], o_s.at[1, c], o_r.at[1, c])
        partial[left, :, higher] = (partial[left, :, higher].astype(F32) + from_right[:, lower].astype(F32)).astype(BF16)
        send(partial.at[left, :, higher], right_done.at[:, higher], c_s.at[1, c], c_r.at[1, c], to_left)
    received(left_done.at[:, high], d_s.at[0], d_r.at[0])
    received(right_done.at[:, low], d_s.at[1], d_r.at[1])
    for c in range(PIECES):
        received(left_done.at[:, pl.ds(c * PIECE, PIECE)], c_s.at[0, c], c_r.at[0, c])
        received(right_done.at[:, pl.ds(HALF + c * PIECE, PIECE)], c_s.at[1, c], c_r.at[1, c])

    @pl.loop(0, BLOCK // 16)
    def _(i):
        at = pl.ds(pl.multiple_of(i * 16, 16), 16)
        projected = partial[x, at, :].astype(F32) + left_done[at, :].astype(F32) + right_done[at, :].astype(F32)
        out[at, :] = (x_raw[x, at, :].astype(F32) + mod_rows[4:5, :] * projected).astype(BF16)

    for copy in sent:
        copy.wait_send()


def shards(
    latent, context, cond, ctx_cond, w_shift, w_scale, w_gate, w_query, key_weight, value_weight, w_out, sink
):
    inverse = (THETA ** (-np.arange(HEAD // 4, dtype=np.float32) * np.float32(2.0) / np.float32(HEAD // 2))).astype(
        np.float32
    )
    inverse = jnp.asarray(np.tile(np.tile(inverse, 4)[None], (8, 1)))
    anywhere = pl.BlockSpec(memory_space=pl.ANY)
    inside = pl.BlockSpec(memory_space=pltpu.VMEM)
    dma = pltpu.SemaphoreType.DMA
    return pl.pallas_call(
        kernel,
        out_shape=jax.ShapeDtypeStruct((BLOCK, WIDTH), BF16),
        in_specs=[anywhere, anywhere, inside, inside]
        + [anywhere] * 7
        + [pl.BlockSpec(memory_space=pltpu.SMEM), inside],
        out_specs=inside,
        scratch_shapes=[
            pltpu.VMEM((NX, BLOCK, WIDTH), BF16),
            pltpu.VMEM((NX * BLOCK, WIDTH), BF16),
            pltpu.VMEM((2, WIDTH, 512), BF16),
            pltpu.VMEM((2, 256, WIDTH), BF16),
            pltpu.VMEM((3, 128, 512), BF16),
            pltpu.VMEM((CTX_ROWS, WIDTH), BF16),
            pltpu.VMEM((CTX_ROWS, WIDTH), BF16),
            pltpu.VMEM((NY, 24, 128), F32),
            pltpu.VMEM((NZ, 24, 128), F32),
            pltpu.VMEM((NT, 24, 128), F32),
            pltpu.VMEM((8, WIDTH), F32),
            pltpu.VMEM((2, 2, NX * BLOCK, 256), BF16),
            pltpu.VMEM((NX, 4, BLOCK, HEAD), BF16),
            pltpu.VMEM((NX + 2, 2, BLOCK, 512), BF16),
            pltpu.VMEM((2, NY, NZ, CTX_ROWS, 256), BF16),
            pltpu.VMEM((NX * BLOCK, 512), BF16),
            pltpu.VMEM((NX, BLOCK, WIDTH), BF16),
            pltpu.VMEM((BLOCK, HALF), BF16),
            pltpu.VMEM((BLOCK, HALF), BF16),
            pltpu.VMEM((BLOCK, WIDTH), BF16),
            pltpu.VMEM((BLOCK, WIDTH), BF16),
            dma((9,)), dma((6,)), dma((6,)), dma((4,)), dma((4,)),
            dma((3,)), dma((3,)), dma((7,)), dma((7,)), dma((7,)), dma((7,)),
            dma((7,)), dma((7,)), dma((3,)), dma((3,)), dma((4,)), dma((4,)),
            dma((4,)), dma((4,)), dma((4,)), dma((4,)),
            dma((2, PIECES)), dma((2, PIECES)), dma((2,)), dma((2,)), dma((2, PIECES)), dma((2, PIECES)),
        ],
        compiler_params=pltpu.CompilerParams(
            collective_id=0, has_side_effects=True, vmem_limit_bytes=60 * 1024 * 1024
        ),
    )(
        latent, context, cond.reshape(NSP, 128), ctx_cond.reshape(NSP, 128), w_shift, w_scale, w_gate,
        w_query, key_weight, value_weight, w_out, sink, inverse,
    )


def solution(mesh):
    in_specs = (
        P(("sp", "tp"), None), P("sp", None), P(), P(), P("sp", "tp"), P("sp", "tp"), P("sp", "tp"),
        P(None, "tp"), P(None, "tp"), P(None, "tp"), P("tp", None), P(),
    )
    out_specs = P(("sp", "tp"), None)
    return jax.shard_map(shards, mesh=mesh, in_specs=in_specs, out_specs=out_specs, check_vma=False)
```

```python
import jax
import jax.numpy as jnp
import numpy as np
from jax import lax
from jax.experimental import pallas as pl
from jax.experimental.pallas import tpu as pltpu
from jax.sharding import PartitionSpec as P

MESH = pl.DeviceIdType.MESH
F32 = jnp.float32
BF16 = jnp.bfloat16

NX, NY, NZ, NT = 4, 4, 8, 8
NSP = NY * NZ
HEAD = 128
SIDE = 128
BLOCK = 64
WIDTH = 4096
HALF = WIDTH // 2
PAIR = 2 * BLOCK
TOKENS = 16384
CTX_ROWS = 32
EPS = 1e-05
THETA = 10000.0
MASKED = -1e30
PIECES = 4
PIECE = HALF // PIECES
ROWS = 16


def kernel(
    latent, context, cond_in, ctx_cond_in, w_shift, w_scale, w_gate, wq, wk, wv, wo, sink_in, inverse_in, out,
    cond, ctx_cond, sink, inverse, cosines, sines, x_raw, means, scales, x_mod, w_all, w_out, w_modulation, ctx_raw, ctx_mod, y_buf, z_buf, t_buf, mod_rows,
    product, query, kv, ckv, attended, partial, from_left, from_right, left_done, right_done,
    l_sem, ag_s, ag_r, w_s, w_r, y_s, y_r, z_s, z_r, t_s, t_r, cz_s, cz_r, cy_s, cy_r, cc_s, cc_r,
    kv_s, kv_r, h_s, h_r, o_s, o_r, d_s, d_r, c_s, c_r,
):
    sp = lax.axis_index("sp")
    tp = lax.axis_index("tp")
    z, y = sp // NY, sp % NY
    x, core = tp // 2, tp % 2
    sibling = x * 2 + 1 - core
    right, opposite, left = (x + 1) % NX, (x + 2) % NX, (x + 3) % NX
    sp_next, sp_back = (sp + 1) % NSP, (sp + NSP - 1) % NSP
    to_right, to_left = (sp, right * 2 + core), (sp, left * 2 + core)
    to_sibling = (sp, sibling)

    def remote(src, dst, send, recv, device):
        return pltpu.make_async_remote_copy(
            src_ref=src, dst_ref=dst, send_sem=send, recv_sem=recv, device_id=device, device_id_type=MESH
        )

    sent = []

    def send(*args):
        copy = remote(*args)
        copy.start()
        sent.append(copy)

    def received(dst, send_sem, recv_sem):
        remote(dst, dst, send_sem, recv_sem, to_sibling).wait_recv()

    local = [
        pltpu.make_async_copy(latent, x_raw.at[x], l_sem.at[0]),
        pltpu.make_async_copy(cond_in, cond, l_sem.at[1]),
        pltpu.make_async_copy(ctx_cond_in, ctx_cond, l_sem.at[2]),
        pltpu.make_async_copy(w_shift, w_modulation.at[0], l_sem.at[3]),
        pltpu.make_async_copy(w_scale, w_modulation.at[1], l_sem.at[4]),
        pltpu.make_async_copy(w_gate, w_modulation.at[2], l_sem.at[5]),
        pltpu.make_async_copy(context, ctx_raw, l_sem.at[6]),
        pltpu.make_async_copy(sink_in, sink, l_sem.at[7]),
        pltpu.make_async_copy(inverse_in, inverse, l_sem.at[8]),
        pltpu.make_async_copy(wq, w_all.at[core, :, 0:256], l_sem.at[9]),
        pltpu.make_async_copy(wk, w_all.at[core, :, 256:384], l_sem.at[10]),
        pltpu.make_async_copy(wv, w_all.at[core, :, 384:512], l_sem.at[11]),
        pltpu.make_async_copy(wo, w_out.at[core], l_sem.at[12]),
    ]
    for copy in local[:6]:
        copy.start()

    barrier = pltpu.get_barrier_semaphore()
    greeted = [(sp, (tp + d) % NT) for d in range(1, NT)]
    greeted += [(z * NY + (y + d) % NY, tp) for d in range(1, NY)]
    greeted += [(((z + d) % NZ) * NY + y, tp) for d in range(1, NZ)]
    greeted += [(sp_next, tp), (sp_next, sibling), (sp_back, tp), (sp_back, sibling)]
    for device in greeted:
        pl.semaphore_signal(barrier, inc=1, device_id=device, device_id_type=MESH)

    local[1].wait()
    local[2].wait()
    act = jnp.concatenate(
        [jax.nn.silu(cond[pl.ds(sp, 1), :]), jax.nn.silu(ctx_cond[pl.ds(sp, 1), :]), jnp.zeros((6, 128), F32)],
        axis=0,
    ).astype(BF16)
    y_buf[y] = jnp.zeros((24, 128), F32)
    for i in range(3):
        local[3 + i].wait()
        part = jnp.dot(act, w_modulation[i], preferred_element_type=F32)
        for row in range(2 if i < 2 else 1):
            for c in range(4):
                at = (2 * i + row) * 4 + c
                y_buf[y, at : at + 1, :] = part[row : row + 1, c * 128 : (c + 1) * 128]

    pl.semaphore_wait(barrier, len(greeted))

    for d in range(1, NY):
        send(y_buf.at[y], y_buf.at[y], y_s.at[d - 1], y_r.at[d - 1], (z * NY + (y + d) % NY, tp))

    local[0].wait()

    def rows_of(piece):
        return pl.ds(piece * ROWS, ROWS)

    def gather(block, piece, i, device):
        ref = x_raw.at[block, rows_of(piece), :]
        send(ref, ref, ag_s.at[i], ag_r.at[i], device)

    def own_pieces(i):
        gather(x, i, i, to_right)
        gather(x, 3 - i, 6 + i, to_left)

    def gathered(i):
        near = i < 4
        if near:
            received(x_raw.at[left, rows_of(i), :], ag_s.at[i], ag_r.at[i])
            received(x_raw.at[right, rows_of(3 - i), :], ag_s.at[6 + i], ag_r.at[6 + i])
        else:
            received(x_raw.at[opposite, rows_of(i - 4), :], ag_s.at[i], ag_r.at[i])
            received(x_raw.at[opposite, rows_of(7 - i), :], ag_s.at[6 + i], ag_r.at[6 + i])

    def forward(i):
        gather(left, i, 4 + i, to_right)
        gather(right, 3 - i, 10 + i, to_left)

    own_pieces(0)
    own_pieces(1)

    for copy in local[6:]:
        copy.start()

    send(wq, w_all.at[core, :, 0:256], w_s.at[0], w_r.at[0], to_sibling)
    send(wk, w_all.at[core, :, 256:384], w_s.at[1], w_r.at[1], to_sibling)
    send(wv, w_all.at[core, :, 384:512], w_s.at[2], w_r.at[2], to_sibling)

    def moments(read, rows):
        chunks = [slice(i * 128, (i + 1) * 128) for i in range(WIDTH // 128)]
        mean = jnp.sum(sum(read(at).astype(F32) for at in chunks), axis=-1, keepdims=True) / WIDTH
        mean = jnp.broadcast_to(mean, (rows, 128))
        var = sum(jnp.square(read(at).astype(F32) - mean) for at in chunks)
        var = jnp.sum(var, axis=-1, keepdims=True) / WIDTH
        return mean, jnp.broadcast_to(lax.rsqrt(var + EPS), (rows, 128))

    def statistics(block, half):
        rows = slice(half * 32, half * 32 + 32)
        means[block, rows, :], scales[block, rows, :] = moments(lambda at: x_raw[block, rows, at], 32)

    @pl.loop(0, 2)
    def _(i):
        at = pl.ds(pl.multiple_of(i * 32, 32), 32)
        means[x, at, :], scales[x, at, :] = moments(lambda columns: x_raw[x, at, columns], 32)

    lane = lax.broadcasted_iota(jnp.int32, (BLOCK, HEAD), 1)
    column = lax.broadcasted_iota(jnp.int32, (BLOCK, HEAD), 0)
    by_row = lane < HEAD // 2
    is_first = lane % (HEAD // 2) < HEAD // 4

    local[7].wait()
    local[8].wait()

    @pl.loop(0, NX)
    def _(b):
        position = jnp.where(by_row, sp * NT + b * 2 + core, column).astype(F32)
        angle = position * inverse[0:1, :]
        cosines[b] = jnp.cos(angle)
        sine = jnp.sin(angle)
        sines[b] = jnp.where(is_first, -sine, sine)

    for d in range(1, NY):
        received(y_buf.at[(y + NY - d) % NY], y_s.at[d - 1], y_r.at[d - 1])
    z_buf[z] = jnp.sum(y_buf[...], axis=0)
    for d in (4, 3, 5, 2, 6, 1, 7):
        send(z_buf.at[z], z_buf.at[z], z_s.at[d - 1], z_r.at[d - 1], (((z + d) % NZ) * NY + y, tp))
    own_pieces(2)
    for d in range(1, NZ):
        received(z_buf.at[(z + NZ - d) % NZ], z_s.at[d - 1], z_r.at[d - 1])
    t_buf[tp] = jnp.sum(z_buf[...], axis=0)
    for d in (4, 5, 3, 2, 6, 7, 1):
        send(t_buf.at[tp], t_buf.at[tp], t_s.at[d - 1], t_r.at[d - 1], (sp, (tp + d) % NT))
    own_pieces(3)
    send(wo, w_out.at[core], w_s.at[3], w_r.at[3], to_sibling)

    for i in range(2):
        gathered(i)
        forward(i)

    statistics(left, 0)
    statistics(right, 1)
    local[6].wait()
    ctx_mean, ctx_scale = moments(lambda at: ctx_raw[:, at], CTX_ROWS)

    for d in range(1, NT):
        received(t_buf.at[(tp + NT - d) % NT], t_s.at[d - 1], t_r.at[d - 1])
    for t in range(NT):
        for row in range(5):
            for c in range(4):
                at = t * 512 + c * 128
                value = t_buf[t, row * 4 + c : row * 4 + c + 1, :]
                mod_rows[row : row + 1, at : at + 128] = 1.0 + value if row in (2, 3) else value

    for i in range(WIDTH // 128):
        at = slice(i * 128, (i + 1) * 128)
        normal = (ctx_raw[:, at].astype(F32) - ctx_mean) * ctx_scale
        ctx_mod[:, at] = (normal * mod_rows[3:4, at] + mod_rows[1:2, at]).astype(BF16)
    for copy in local[9:]:
        copy.wait()
    halves = [
        jnp.dot(ctx_mod[:, at], w_all[core, at, 256:512], preferred_element_type=F32)
        for at in (slice(0, HALF), slice(HALF, WIDTH))
    ]
    ckv[core, y, z] = (halves[0] + halves[1]).astype(BF16)

    def spread(d):
        line = ckv.at[core, y, (z + NZ - d) % NZ]
        if d:
            received(line, cz_s.at[d - 1], cz_r.at[d - 1])
        for e in (2, 1, 3):
            send(line, line, cy_s.at[d, e - 1], cy_r.at[d, e - 1], (z * NY + (y + e) % NY, tp))
        send(line, line, cc_s.at[d, 0], cc_r.at[d, 0], to_sibling)

    def relay(d):
        for e in range(1, NY):
            line = ckv.at[core, (y + NY - e) % NY, (z + NZ - d) % NZ]
            received(line, cy_s.at[d, e - 1], cy_r.at[d, e - 1])
            send(line, line, cc_s.at[d, e], cc_r.at[d, e], to_sibling)

    own = ckv.at[core, y, z]
    for d in (4, 3, 5, 2, 6, 1, 7):
        send(own, own, cz_s.at[d - 1], cz_r.at[d - 1], (((z + d) % NZ) * NY + y, tp))
    spread(0)

    blocks = (x, right, left, opposite)

    def modulate(slot):
        block = blocks[slot]

        @pl.loop(0, WIDTH // 512)
        def _(c):
            for q in range(4):
                at = pl.ds(pl.multiple_of(c * 512 + q * 128, 128), 128)
                normal = (x_raw[block, :, at].astype(F32) - means[block]) * scales[block]
                x_mod[slot * BLOCK : (slot + 1) * BLOCK, at] = (
                    normal * mod_rows[2:3, at] + mod_rows[0:1, at]
                ).astype(BF16)

    modulate(0)
    gathered(2)
    gathered(3)

    statistics(left, 1)
    statistics(right, 0)

    modulate(1)
    modulate(2)

    def project(c, slot, slots):
        rows = slice(slot * BLOCK, (slot + slots) * BLOCK)
        for j in range(2):
            product[j, c, rows, :] = jnp.dot(
                x_mod[rows, :], w_all[j, :, c * 256 : (c + 1) * 256], preferred_element_type=F32
            ).astype(BF16)

    def place(slot):
        return (x + slot + slot // 2 * (5 - 2 * slot)) % NX, pl.ds(pl.multiple_of(slot * BLOCK, BLOCK), BLOCK)

    def turned(value, b):
        value = value.astype(F32)
        partner = jnp.where(is_first, pltpu.roll(value, 96, 1), pltpu.roll(value, 32, 1))
        return (value * cosines[b] + partner * sines[b]).astype(BF16)

    def turn_keys(slot):
        b, rows = place(slot)
        for j in range(2):
            kv[b + 1, core, :, j * HEAD : (j + 1) * HEAD] = turned(product[j, 1, rows, 0:HEAD], b)
            kv[b + 1, core, :, (2 + j) * HEAD : (3 + j) * HEAD] = product[j, 1, rows, HEAD : 2 * HEAD]

    def turn_queries(slot):
        b, rows = place(slot)
        for j in range(2):
            for g in range(2):
                query[b, 2 * j + g] = turned(product[j, 0, rows, g * HEAD : (g + 1) * HEAD], b)

    def share(slot):
        ref = kv.at[blocks[slot] + 1, core]
        send(ref, ref, kv_s.at[slot], kv_r.at[slot], to_sibling)

    halo = []
    for k, tp_there in enumerate((tp, sibling)):
        halo.append(remote(kv.at[NX, core], kv.at[0, core], h_s.at[k], h_r.at[k], (sp_next, tp_there)))
    for k, tp_there in enumerate((tp, sibling)):
        halo.append(remote(kv.at[1, core], kv.at[NX + 1, core], h_s.at[2 + k], h_r.at[2 + k], (sp_back, tp_there)))
    sent.extend(halo)

    def halo_when(last_late, first_late):
        @pl.when(last_late)
        def _():
            halo[0].start()
            halo[1].start()

        @pl.when(first_late)
        def _():
            halo[2].start()
            halo[3].start()

    other = w_all.at[1 - core]
    received(other.at[:, 0:256], w_s.at[0], w_r.at[0])
    received(other.at[:, 256:384], w_s.at[1], w_r.at[1])
    received(other.at[:, 384:512], w_s.at[2], w_r.at[2])
    project(1, 0, 3)
    for d in (1, 7, 2, 6):
        spread(d)

    @pl.loop(0, 3)
    def _(slot):
        turn_keys(slot)

    for slot in range(3):
        share(slot)
    halo_when(opposite != NX - 1, opposite != 0)
    project(0, 0, 3)
    for d in (3, 5, 4):
        spread(d)

    @pl.loop(0, 3)
    def _(slot):
        turn_queries(slot)

    gathered(4)
    gathered(5)

    statistics(opposite, 0)
    statistics(opposite, 1)
    modulate(3)
    project(1, 3, 1)
    turn_keys(3)
    share(3)
    halo_when(opposite == NX - 1, opposite == 0)
    for d in (0, 1, 7):
        relay(d)
    project(0, 3, 1)
    turn_queries(3)
    for d in (2, 6, 3, 5, 4):
        relay(d)
    for slot in (0, 1, 2, 3):
        received(kv.at[blocks[slot] + 1, 1 - core], kv_s.at[slot], kv_r.at[slot])
    for d in range(NZ):
        for e in range(NY):
            received(ckv.at[1 - core, (y + NY - e) % NY, (z + NZ - d) % NZ], cc_s.at[d, e], cc_r.at[d, e])
    for k, core_there in enumerate((core, 1 - core)):
        received(kv.at[0, core_there], h_s.at[k], h_r.at[k])
        received(kv.at[NX + 1, core_there], h_s.at[2 + k], h_r.at[2 + k])

    factor = HEAD ** (-0.5)
    i_query = lax.broadcasted_iota(jnp.int32, (PAIR, 3 * PAIR), 0) % BLOCK + core * BLOCK
    i_key = lax.broadcasted_iota(jnp.int32, (PAIR, 3 * PAIR), 1) - PAIR
    near = jnp.abs(i_key - i_query) <= SIDE
    upper = lax.broadcasted_iota(jnp.int32, (PAIR, 1), 0) < BLOCK
    across = (((1,), (1,)), ((), ()))

    def attend(b, slot):
        key_at = i_key + (sp * NT * BLOCK + b * PAIR)
        valid = near & (key_at >= 0) & (key_at < TOKENS)
        for h in range(2):
            q = query[b, 2 * h : 2 * h + 2].reshape(PAIR, HEAD)
            k_band = kv[pl.ds(b, 3), :, :, h * HEAD : (h + 1) * HEAD].reshape(3 * PAIR, HEAD)
            v_band = kv[pl.ds(b, 3), :, :, (2 + h) * HEAD : (3 + h) * HEAD].reshape(3 * PAIR, HEAD)
            k_ctx = ckv[h, :, :, :, 0:HEAD].reshape(NSP * CTX_ROWS, HEAD)
            v_ctx = ckv[h, :, :, :, HEAD : 2 * HEAD].reshape(NSP * CTX_ROWS, HEAD)
            s_band = lax.dot_general(q, k_band, across, preferred_element_type=F32) * factor
            s_band = jnp.where(valid, s_band, MASKED)
            s_ctx = lax.dot_general(q, k_ctx, across, preferred_element_type=F32) * factor
            sinks = jnp.where(upper, sink[4 * x + 2 * h], sink[4 * x + 2 * h + 1])
            top = jnp.maximum(
                jnp.maximum(jnp.max(s_band, axis=-1, keepdims=True), jnp.max(s_ctx, axis=-1, keepdims=True)), sinks
            )
            e_band = jnp.exp(s_band - top)
            e_ctx = jnp.exp(s_ctx - top)
            total = (
                jnp.sum(e_band, axis=-1, keepdims=True)
                + jnp.sum(e_ctx, axis=-1, keepdims=True)
                + jnp.exp(sinks - top)
            )
            value = jnp.dot(e_band.astype(BF16), v_band, preferred_element_type=F32)
            value += jnp.dot(e_ctx.astype(BF16), v_ctx, preferred_element_type=F32)
            value = (value / total).astype(BF16)
            rows = slice(slot * BLOCK, (slot + 1) * BLOCK)
            for g in range(2):
                attended[rows, (2 * h + g) * HEAD : (2 * h + g + 1) * HEAD] = value[g * BLOCK : (g + 1) * BLOCK]

    def output(slot, slots, at, width):
        rows = slice(slot * BLOCK, (slot + slots) * BLOCK)
        columns = slice(at, at + width)
        result = jnp.dot(attended[rows, 0:256], w_out[0, :, columns], preferred_element_type=F32)
        result += jnp.dot(attended[rows, 256:512], w_out[1, :, columns], preferred_element_type=F32)
        result = result.astype(BF16)
        for s in range(slots):
            partial[slot + s, :, columns] = result[s * BLOCK : (s + 1) * BLOCK]

    attend(opposite, 3)
    received(w_out.at[1 - core], w_s.at[3], w_r.at[3])
    for c in range(PIECES):
        output(3, 1, c * PIECE, PIECE)
        output(3, 1, HALF + c * PIECE, PIECE)
        lower = pl.ds(c * PIECE, PIECE)
        higher = pl.ds(HALF + c * PIECE, PIECE)
        send(partial.at[3, :, lower], from_left.at[:, lower], o_s.at[0, c], o_r.at[0, c], to_right)
        send(partial.at[3, :, higher], from_right.at[:, lower], o_s.at[1, c], o_r.at[1, c], to_left)
    attend(right, 1)
    attend(left, 2)
    for c in range(2 * PIECES):
        output(1, 2, c * PIECE, PIECE)
    low, high = pl.ds(0, HALF), pl.ds(HALF, HALF)
    send(partial.at[1, :, high], left_done.at[:, high], d_s.at[0], d_r.at[0], to_right)
    send(partial.at[2, :, low], right_done.at[:, low], d_s.at[1], d_r.at[1], to_left)
    for c in range(PIECES):
        lower = pl.ds(c * PIECE, PIECE)
        higher = pl.ds(HALF + c * PIECE, PIECE)
        received(from_left.at[:, lower], o_s.at[0, c], o_r.at[0, c])
        partial[1, :, lower] = (partial[1, :, lower].astype(F32) + from_left[:, lower].astype(F32)).astype(BF16)
        send(partial.at[1, :, lower], left_done.at[:, lower], c_s.at[0, c], c_r.at[0, c], to_right)
        received(from_right.at[:, lower], o_s.at[1, c], o_r.at[1, c])
        partial[2, :, higher] = (partial[2, :, higher].astype(F32) + from_right[:, lower].astype(F32)).astype(BF16)
        send(partial.at[2, :, higher], right_done.at[:, higher], c_s.at[1, c], c_r.at[1, c], to_left)
    attend(x, 0)
    for c in range(2 * PIECES):
        output(0, 1, c * PIECE, PIECE)
    received(left_done.at[:, high], d_s.at[0], d_r.at[0])
    received(right_done.at[:, low], d_s.at[1], d_r.at[1])
    for c in range(PIECES):
        received(left_done.at[:, pl.ds(c * PIECE, PIECE)], c_s.at[0, c], c_r.at[0, c])
        received(right_done.at[:, pl.ds(HALF + c * PIECE, PIECE)], c_s.at[1, c], c_r.at[1, c])

    @pl.loop(0, BLOCK // ROWS)
    def _(i):
        at = pl.ds(pl.multiple_of(i * ROWS, ROWS), ROWS)
        projected = partial[0, at, :].astype(F32) + left_done[at, :].astype(F32) + right_done[at, :].astype(F32)
        out[at, :] = (x_raw[x, at, :].astype(F32) + mod_rows[4:5, :] * projected).astype(BF16)

    for copy in sent:
        copy.wait_send()


def shards(
    latent, context, cond, ctx_cond, w_shift, w_scale, w_gate, w_query, key_weight, value_weight, w_out, sink
):
    inverse = (THETA ** (-np.arange(HEAD // 4, dtype=np.float32) * np.float32(2.0) / np.float32(HEAD // 2))).astype(
        np.float32
    )
    inverse = jnp.asarray(np.tile(np.tile(inverse, 4)[None], (8, 1)))
    anywhere = pl.BlockSpec(memory_space=pl.ANY)
    inside = pl.BlockSpec(memory_space=pltpu.VMEM)
    dma = pltpu.SemaphoreType.DMA
    return pl.pallas_call(
        kernel,
        out_shape=pltpu.VMEM((BLOCK, WIDTH), BF16),
        in_specs=[anywhere] * 13,
        out_specs=inside,
        scratch_shapes=[
            pltpu.VMEM((NSP, 128), F32),
            pltpu.VMEM((NSP, 128), F32),
            pltpu.SMEM((16,), F32),
            pltpu.VMEM((8, 128), F32),
            pltpu.VMEM((NX, BLOCK, HEAD), F32),
            pltpu.VMEM((NX, BLOCK, HEAD), F32),
            pltpu.VMEM((NX, BLOCK, WIDTH), BF16),
            pltpu.VMEM((NX, BLOCK, 128), F32),
            pltpu.VMEM((NX, BLOCK, 128), F32),
            pltpu.VMEM((NX * BLOCK, WIDTH), BF16),
            pltpu.VMEM((2, WIDTH, 512), BF16),
            pltpu.VMEM((2, 256, WIDTH), BF16),
            pltpu.VMEM((3, 128, 512), BF16),
            pltpu.VMEM((CTX_ROWS, WIDTH), BF16),
            pltpu.VMEM((CTX_ROWS, WIDTH), BF16),
            pltpu.VMEM((NY, 24, 128), F32),
            pltpu.VMEM((NZ, 24, 128), F32),
            pltpu.VMEM((NT, 24, 128), F32),
            pltpu.VMEM((8, WIDTH), F32),
            pltpu.VMEM((2, 2, NX * BLOCK, 256), BF16),
            pltpu.VMEM((NX, 4, BLOCK, HEAD), BF16),
            pltpu.VMEM((NX + 2, 2, BLOCK, 512), BF16),
            pltpu.VMEM((2, NY, NZ, CTX_ROWS, 256), BF16),
            pltpu.VMEM((NX * BLOCK, 512), BF16),
            pltpu.VMEM((NX, BLOCK, WIDTH), BF16),
            pltpu.VMEM((BLOCK, HALF), BF16),
            pltpu.VMEM((BLOCK, HALF), BF16),
            pltpu.VMEM((BLOCK, WIDTH), BF16),
            pltpu.VMEM((BLOCK, WIDTH), BF16),
            dma((13,)), dma((12,)), dma((12,)), dma((4,)), dma((4,)),
            dma((3,)), dma((3,)), dma((7,)), dma((7,)), dma((7,)), dma((7,)),
            dma((7,)), dma((7,)), dma((8, 3)), dma((8, 3)), dma((8, 4)), dma((8, 4)),
            dma((4,)), dma((4,)), dma((4,)), dma((4,)),
            dma((2, PIECES)), dma((2, PIECES)), dma((2,)), dma((2,)), dma((2, PIECES)), dma((2, PIECES)),
        ],
        compiler_params=pltpu.CompilerParams(
            collective_id=0, has_side_effects=True, vmem_limit_bytes=60 * 1024 * 1024
        ),
    )(
        latent, context, cond.reshape(NSP, 128), ctx_cond.reshape(NSP, 128), w_shift, w_scale, w_gate,
        w_query, key_weight, value_weight, w_out, sink, inverse,
    )


def solution(mesh):
    in_specs = (
        P(("sp", "tp"), None), P("sp", None), P(), P(), P("sp", "tp"), P("sp", "tp"), P("sp", "tp"),
        P(None, "tp"), P(None, "tp"), P(None, "tp"), P("tp", None), P(),
    )
    out_specs = P(("sp", "tp"), None)
    return jax.shard_map(shards, mesh=mesh, in_specs=in_specs, out_specs=out_specs, check_vma=False)
```

```python
import jax
import jax.numpy as jnp
import numpy as np
from jax import lax
from jax.experimental import pallas as pl
from jax.experimental.pallas import tpu as pltpu
from jax.sharding import PartitionSpec as P

MESH = pl.DeviceIdType.MESH
F32 = jnp.float32
BF16 = jnp.bfloat16

NX, NY, NZ, NT = 4, 4, 8, 8
NSP = NY * NZ
HEAD = 128
SIDE = 128
BLOCK = 64
WIDTH = 4096
HALF = WIDTH // 2
PAIR = 2 * BLOCK
TOKENS = 16384
CTX_ROWS = 32
EPS = 1e-05
THETA = 10000.0
MASKED = -1e30
PIECES = 4
PIECE = HALF // PIECES
ROWS = 16
SINGLE = 34


def kernel(
    latent, context, cond_in, ctx_cond_in, w_shift, w_scale, w_gate, wq, wk, wv, wo, sink_in, inverse_in, out,
    cond, ctx_cond, sink, inverse, cosines, sines, x_raw, means, scales, x_mod, w_all, w_out, w_modulation, ctx_raw, ctx_mod, y_buf, z_buf, t_buf, zg_buf, tg_buf, mod_rows,
    product, query, kv, ckv, attended, partial, from_left, from_right, left_done, right_done,
    l_sem, ag_r, cz_r, cy_r, h_r, o_r, sems,
):
    sp = lax.axis_index("sp")
    tp = lax.axis_index("tp")
    z, y = sp // NY, sp % NY
    x, core = tp // 2, tp % 2
    sibling = x * 2 + 1 - core
    right, opposite, left = (x + 1) % NX, (x + 2) % NX, (x + 3) % NX
    sp_next, sp_back = (sp + 1) % NSP, (sp + NSP - 1) % NSP
    to_right, to_left = (sp, right * 2 + core), (sp, left * 2 + core)
    to_sibling = (sp, sibling)

    def remote(src, dst, send, recv, device):
        return pltpu.make_async_remote_copy(
            src_ref=src, dst_ref=dst, send_sem=send, recv_sem=recv, device_id=device, device_id_type=MESH
        )

    names = iter(range(SINGLE))

    def pair():
        return sems.at[next(names)], sems.at[next(names)]

    def send(*args):
        remote(*args).start()

    def received(ref, sem):
        remote(ref, ref, sem, sem, to_sibling).wait_recv()

    drains = []

    def drained_at_end(ref, sem):
        drains.append(remote(ref, ref, sem, sem, to_sibling))

    local = [
        pltpu.make_async_copy(cond_in, cond, l_sem.at[0]),
        pltpu.make_async_copy(ctx_cond_in, ctx_cond, l_sem.at[1]),
        pltpu.make_async_copy(w_shift, w_modulation.at[0], l_sem.at[2]),
        pltpu.make_async_copy(w_scale, w_modulation.at[1], l_sem.at[3]),
        pltpu.make_async_copy(w_gate, w_modulation.at[2], l_sem.at[4]),
        pltpu.make_async_copy(latent, x_raw.at[x], l_sem.at[5]),
        pltpu.make_async_copy(context, ctx_raw, l_sem.at[6]),
        pltpu.make_async_copy(sink_in, sink, l_sem.at[7]),
        pltpu.make_async_copy(inverse_in, inverse, l_sem.at[8]),
        pltpu.make_async_copy(wq, w_all.at[core, :, 0:256], l_sem.at[9]),
        pltpu.make_async_copy(wk, w_all.at[core, :, 256:384], l_sem.at[10]),
        pltpu.make_async_copy(wv, w_all.at[core, :, 384:512], l_sem.at[11]),
        pltpu.make_async_copy(wo, w_out.at[core], l_sem.at[12]),
    ]
    for copy in local[:6]:
        copy.start()

    barrier = pltpu.get_barrier_semaphore()
    greeted = [(sp, (tp + d) % NT) for d in range(1, NT)]
    greeted += [(z * NY + (y + d) % NY, tp) for d in range(1, NY)]
    greeted += [(((z + d) % NZ) * NY + y, tp) for d in range(1, NZ)]
    greeted += [(sp_next, tp), (sp_next, sibling), (sp_back, tp), (sp_back, sibling)]
    for device in greeted:
        pl.semaphore_signal(barrier, inc=1, device_id=device, device_id_type=MESH)

    local[0].wait()
    local[1].wait()
    act = jnp.concatenate(
        [jax.nn.silu(cond[pl.ds(sp, 1), :]), jax.nn.silu(ctx_cond[pl.ds(sp, 1), :]), jnp.zeros((6, 128), F32)],
        axis=0,
    ).astype(BF16)
    y_buf[y] = jnp.zeros((24, 128), F32)
    for i in range(3):
        local[2 + i].wait()
        part = jnp.dot(act, w_modulation[i], preferred_element_type=F32)
        for row in range(2 if i < 2 else 1):
            for c in range(4):
                at = (2 * i + row) * 4 + c
                y_buf[y, at : at + 1, :] = part[row : row + 1, c * 128 : (c + 1) * 128]

    pl.semaphore_wait(barrier, len(greeted))

    y_s, y_r = pair()
    for d in range(1, NY):
        send(y_buf.at[y], y_buf.at[y], y_s, y_r, (z * NY + (y + d) % NY, tp))
    drained_at_end(y_buf.at[0:3], y_s)

    local[5].wait()
    ag_s, _ = pair()
    drained_at_end(x_raw.at[0:3], ag_s)

    def rows_of(piece):
        return pl.ds(piece * ROWS, ROWS)

    def gather(block, piece, i, device):
        ref = x_raw.at[block, rows_of(piece), :]
        send(ref, ref, ag_s, ag_r.at[i], device)

    def own_pieces(i):
        gather(x, i, i, to_right)
        gather(x, 3 - i, 6 + i, to_left)

    def gathered(i):
        near = i < 4
        if near:
            received(x_raw.at[left, rows_of(i), :], ag_r.at[i])
            received(x_raw.at[right, rows_of(3 - i), :], ag_r.at[6 + i])
        else:
            received(x_raw.at[opposite, rows_of(i - 4), :], ag_r.at[i])
            received(x_raw.at[opposite, rows_of(7 - i), :], ag_r.at[6 + i])

    def forward(i):
        gather(left, i, 4 + i, to_right)
        gather(right, 3 - i, 10 + i, to_left)

    own_pieces(0)
    own_pieces(1)

    for copy in local[6:]:
        copy.start()

    w_s, w_r = pair()
    send(wq, w_all.at[core, :, 0:256], w_s, w_r, to_sibling)
    send(wk, w_all.at[core, :, 256:384], w_s, w_r, to_sibling)
    send(wv, w_all.at[core, :, 384:512], w_s, w_r, to_sibling)
    drained_at_end(w_all.at[core], w_s)

    def moments(read, rows):
        chunks = [slice(i * 128, (i + 1) * 128) for i in range(WIDTH // 128)]
        mean = jnp.sum(sum(read(at).astype(F32) for at in chunks), axis=-1, keepdims=True) / WIDTH
        mean = jnp.broadcast_to(mean, (rows, 128))
        var = sum(jnp.square(read(at).astype(F32) - mean) for at in chunks)
        var = jnp.sum(var, axis=-1, keepdims=True) / WIDTH
        return mean, jnp.broadcast_to(lax.rsqrt(var + EPS), (rows, 128))

    def statistics(block, half):
        rows = slice(half * 32, half * 32 + 32)
        means[block, rows, :], scales[block, rows, :] = moments(lambda at: x_raw[block, rows, at], 32)

    @pl.loop(0, 2)
    def _(i):
        at = pl.ds(pl.multiple_of(i * 32, 32), 32)
        means[x, at, :], scales[x, at, :] = moments(lambda columns: x_raw[x, at, columns], 32)

    lane = lax.broadcasted_iota(jnp.int32, (BLOCK, HEAD), 1)
    column = lax.broadcasted_iota(jnp.int32, (BLOCK, HEAD), 0)
    by_row = lane < HEAD // 2
    is_first = lane % (HEAD // 2) < HEAD // 4

    local[7].wait()
    local[8].wait()

    @pl.loop(0, NX)
    def _(b):
        position = jnp.where(by_row, sp * NT + b * 2 + core, column).astype(F32)
        angle = position * inverse[0:1, :]
        cosines[b] = jnp.cos(angle)
        sine = jnp.sin(angle)
        sines[b] = jnp.where(is_first, -sine, sine)

    received(y_buf.at[0:3], y_r)
    total = jnp.sum(y_buf[...], axis=0)
    z_buf[z] = total[0:16]
    zg_buf[z] = total[16:24]
    z_s, z_r = pair()
    for d in (4, 3, 5, 2, 6, 1, 7):
        send(z_buf.at[z], z_buf.at[z], z_s, z_r, (((z + d) % NZ) * NY + y, tp))
    drained_at_end(z_buf.at[0:7], z_s)
    own_pieces(2)
    received(z_buf.at[0:7], z_r)
    t_buf[tp] = jnp.sum(z_buf[...], axis=0)
    t_s, t_r = pair()
    for d in (4, 5, 3, 2, 6, 7, 1):
        send(t_buf.at[tp], t_buf.at[tp], t_s, t_r, (sp, (tp + d) % NT))
    drained_at_end(t_buf.at[0:7], t_s)
    own_pieces(3)
    zg_s, zg_r = pair()
    for d in range(1, NZ):
        send(zg_buf.at[z], zg_buf.at[z], zg_s, zg_r, (((z + d) % NZ) * NY + y, tp))
    drained_at_end(zg_buf.at[0:7], zg_s)
    wo_s, wo_r = pair()
    send(wo, w_out.at[core], wo_s, wo_r, to_sibling)
    drained_at_end(w_out.at[core], wo_s)

    for i in range(2):
        gathered(i)
        forward(i)

    statistics(left, 0)
    statistics(right, 1)
    local[6].wait()
    ctx_mean, ctx_scale = moments(lambda at: ctx_raw[:, at], CTX_ROWS)

    received(t_buf.at[0:7], t_r)
    for t in range(NT):
        values = t_buf[t]
        for row in range(4):
            for c in range(4):
                at = t * 512 + c * 128
                value = values[row * 4 + c : row * 4 + c + 1, :]
                mod_rows[row : row + 1, at : at + 128] = 1.0 + value if row > 1 else value

    for i in range(WIDTH // 128):
        at = slice(i * 128, (i + 1) * 128)
        normal = (ctx_raw[:, at].astype(F32) - ctx_mean) * ctx_scale
        ctx_mod[:, at] = (normal * mod_rows[3:4, at] + mod_rows[1:2, at]).astype(BF16)
    for copy in local[9:]:
        copy.wait()
    halves = [
        jnp.dot(ctx_mod[:, at], w_all[core, at, 256:512], preferred_element_type=F32)
        for at in (slice(0, HALF), slice(HALF, WIDTH))
    ]
    ckv[core, y, z] = (halves[0] + halves[1]).astype(BF16)

    cz_s, _ = pair()
    cy_s, cw_s = pair()
    cc_s, cc_r = pair()

    near_z = (1, 7, 2, 6)

    def spread(d):
        line = ckv.at[core, y, (z + NZ - d) % NZ]
        if d:
            received(line, cz_r.at[d - 1])
        if d not in near_z:
            for e in (2, 1, 3):
                send(line, line, cy_s, cy_r.at[d], (z * NY + (y + e) % NY, tp))
        send(line, line, cc_s, cc_r, to_sibling)

    def relay(d):
        there = (z + NZ - d) % NZ
        received(ckv.at[core, 0:3, there], cy_r.at[d])
        for e in range(1, NY):
            line = ckv.at[core, (y + NY - e) % NY, there]
            if d == 0:
                for f in near_z:
                    send(line, line, cw_s, cy_r.at[f], (((z + f) % NZ) * NY + y, tp))
            send(line, line, cc_s, cc_r, to_sibling)

    own = ckv.at[core, y, z]
    for d in (4, 3, 5, 2, 6, 1, 7):
        send(own, own, cz_s, cz_r.at[d - 1], (((z + d) % NZ) * NY + y, tp))
    drained_at_end(ckv.at[core, 0, 0:7], cz_s)
    drained_at_end(ckv.at[0, 0:3, 0:4], cy_s)
    drained_at_end(ckv.at[0, 0:3, 0:4], cw_s)
    drained_at_end(ckv.at[core], cc_s)
    spread(0)

    blocks = (x, right, left, opposite)

    def modulate(slot):
        block = blocks[slot]

        @pl.loop(0, WIDTH // 512)
        def _(c):
            for q in range(4):
                at = pl.ds(pl.multiple_of(c * 512 + q * 128, 128), 128)
                normal = (x_raw[block, :, at].astype(F32) - means[block]) * scales[block]
                x_mod[slot * BLOCK : (slot + 1) * BLOCK, at] = (
                    normal * mod_rows[2:3, at] + mod_rows[0:1, at]
                ).astype(BF16)

    modulate(0)
    gathered(2)
    gathered(3)

    statistics(left, 1)
    statistics(right, 0)

    modulate(1)
    modulate(2)

    def project(c, slot, slots):
        rows = slice(slot * BLOCK, (slot + slots) * BLOCK)
        for j in range(2):
            product[j, c, rows, :] = jnp.dot(
                x_mod[rows, :], w_all[j, :, c * 256 : (c + 1) * 256], preferred_element_type=F32
            ).astype(BF16)

    def place(slot):
        return (x + slot + slot // 2 * (5 - 2 * slot)) % NX, pl.ds(pl.multiple_of(slot * BLOCK, BLOCK), BLOCK)

    def turned(value, b):
        value = value.astype(F32)
        partner = jnp.where(is_first, pltpu.roll(value, 96, 1), pltpu.roll(value, 32, 1))
        return (value * cosines[b] + partner * sines[b]).astype(BF16)

    def turn_keys(slot):
        b, rows = place(slot)
        for j in range(2):
            kv[b + 1, core, j] = turned(product[j, 1, rows, 0:HEAD], b)
            kv[b + 1, core, 2 + j] = product[j, 1, rows, HEAD : 2 * HEAD]

    def turn_queries(slot):
        b, rows = place(slot)
        for j in range(2):
            for g in range(2):
                query[b, 2 * j + g] = turned(product[j, 0, rows, g * HEAD : (g + 1) * HEAD], b)

    kv_s, kv_r = pair()
    drained_at_end(kv.at[1:5, core], kv_s)

    def share(slot):
        ref = kv.at[blocks[slot] + 1, core]
        send(ref, ref, kv_s, kv_r, to_sibling)

    h_s, _ = pair()
    drained_at_end(kv.at[1:4, core], h_s)
    to_next = remote(kv.at[NX, core], kv.at[0, core], h_s, h_r.at[0], (sp_next, tp))
    to_back = remote(kv.at[1, core], kv.at[NX + 1, core], h_s, h_r.at[2], (sp_back, tp))
    to_next_other = remote(kv.at[NX, core], kv.at[0, core], h_s, h_r.at[1], (sp_next, sibling))
    to_back_other = remote(kv.at[1, core], kv.at[NX + 1, core], h_s, h_r.at[3], (sp_back, sibling))
    kv[(NX + 1) * (1 - core), 1 - core] = jnp.zeros((4, BLOCK, HEAD), BF16)

    def halo_when(last, first):
        @pl.when(last)
        def _():
            to_next.start()

            @pl.when(core == 1)
            def _():
                to_next_other.start()

        @pl.when(first)
        def _():
            to_back.start()

            @pl.when(core == 0)
            def _():
                to_back_other.start()

    def halo_received(first, last):
        @pl.when(first)
        def _():
            received(kv.at[0, core], h_r.at[0])

            @pl.when(core == 0)
            def _():
                received(kv.at[0, 1], h_r.at[1])

        @pl.when(last)
        def _():
            received(kv.at[NX + 1, core], h_r.at[2])

            @pl.when(core == 1)
            def _():
                received(kv.at[NX + 1, 0], h_r.at[3])

    other = w_all.at[1 - core]
    received(other, w_r)
    project(1, 0, 3)
    relay(0)

    @pl.loop(0, 3)
    def _(slot):
        turn_keys(slot)

    for slot in range(3):
        share(slot)
    halo_when(opposite != NX - 1, opposite != 0)
    for d in (3, 5, 4, 1, 7, 2, 6):
        spread(d)
    project(0, 0, 3)

    @pl.loop(0, 3)
    def _(slot):
        turn_queries(slot)

    gathered(4)
    gathered(5)

    received(zg_buf.at[0:7], zg_r)
    tg_buf[tp] = jnp.sum(zg_buf[...], axis=0)
    tg_s, tg_r = pair()
    for d in range(1, NT):
        send(tg_buf.at[tp], tg_buf.at[tp], tg_s, tg_r, (sp, (tp + d) % NT))
    drained_at_end(tg_buf.at[0:7], tg_s)

    statistics(opposite, 0)
    statistics(opposite, 1)
    modulate(3)
    project(1, 3, 1)
    turn_keys(3)
    share(3)
    halo_when(opposite == NX - 1, opposite == 0)
    for d in (1, 7, 2, 6):
        relay(d)
    project(0, 3, 1)
    turn_queries(3)
    for d in (3, 5, 4):
        relay(d)
    received(kv.at[1:5, 1 - core], kv_r)
    halo_received(opposite == 0, opposite == NX - 1)

    factor = HEAD ** (-0.5)
    i_query = lax.broadcasted_iota(jnp.int32, (PAIR, 3 * PAIR), 0) % BLOCK + core * BLOCK
    i_key = lax.broadcasted_iota(jnp.int32, (PAIR, 3 * PAIR), 1) - PAIR
    near = jnp.abs(i_key - i_query) <= SIDE
    upper = lax.broadcasted_iota(jnp.int32, (PAIR, 1), 0) < BLOCK
    across = (((1,), (1,)), ((), ()))

    def attend(b, slot, heads=(0, 1)):
        key_at = i_key + (sp * NT * BLOCK + b * PAIR)
        valid = near & (key_at >= 0) & (key_at < TOKENS)
        for h in heads:
            q = query[b, pl.ds(2 * h, 2)].reshape(PAIR, HEAD)
            k_band = kv[pl.ds(b, 3), :, h].reshape(3 * PAIR, HEAD)
            v_band = kv[pl.ds(b, 3), :, 2 + h].reshape(3 * PAIR, HEAD)
            k_ctx = ckv[h, :, :, :, 0:HEAD].reshape(NSP * CTX_ROWS, HEAD)
            v_ctx = ckv[h, :, :, :, HEAD : 2 * HEAD].reshape(NSP * CTX_ROWS, HEAD)
            s_band = lax.dot_general(q, k_band, across, preferred_element_type=F32) * factor
            s_band = jnp.where(valid, s_band, MASKED)
            s_ctx = lax.dot_general(q, k_ctx, across, preferred_element_type=F32) * factor
            sinks = jnp.where(upper, sink[4 * x + 2 * h], sink[4 * x + 2 * h + 1])
            top = jnp.maximum(
                jnp.maximum(jnp.max(s_band, axis=-1, keepdims=True), jnp.max(s_ctx, axis=-1, keepdims=True)), sinks
            )
            e_band = jnp.exp(s_band - top)
            e_ctx = jnp.exp(s_ctx - top)
            total = (
                jnp.sum(e_band, axis=-1, keepdims=True)
                + jnp.sum(e_ctx, axis=-1, keepdims=True)
                + jnp.exp(sinks - top)
            )
            value = jnp.dot(e_band.astype(BF16), v_band, preferred_element_type=F32)
            value += jnp.dot(e_ctx.astype(BF16), v_ctx, preferred_element_type=F32)
            value = (value / total).astype(BF16)
            rows = slice(slot * BLOCK, (slot + 1) * BLOCK)
            for g in range(2):
                attended[h, rows, g * HEAD : (g + 1) * HEAD] = value[g * BLOCK : (g + 1) * BLOCK]

    def output(slot, slots, at, width):
        rows = slice(slot * BLOCK, (slot + slots) * BLOCK)
        columns = slice(at, at + width)
        result = jnp.dot(attended[0, rows, :], w_out[0, :, columns], preferred_element_type=F32)
        result += jnp.dot(attended[1, rows, :], w_out[1, :, columns], preferred_element_type=F32)
        result = result.astype(BF16)
        for s in range(slots):
            partial[slot + s, :, columns] = result[s * BLOCK : (s + 1) * BLOCK]

    attend(opposite, 3, (core,))
    received(ckv.at[1 - core], cc_r)
    attend(opposite, 3, (1 - core,))
    received(w_out.at[1 - core], wo_r)
    o_s, d_s = pair()
    c_s, _ = pair()
    left_r, right_r = pair()
    for sem in (o_s, d_s, c_s):
        drained_at_end(partial.at[0], sem)
    for c in range(PIECES):
        output(3, 1, c * PIECE, PIECE)
        output(3, 1, HALF + c * PIECE, PIECE)
        lower = pl.ds(c * PIECE, PIECE)
        higher = pl.ds(HALF + c * PIECE, PIECE)
        send(partial.at[3, :, lower], from_left.at[:, lower], o_s, o_r.at[0, c], to_right)
        send(partial.at[3, :, higher], from_right.at[:, lower], o_s, o_r.at[1, c], to_left)
    halo_received(opposite != 0, opposite != NX - 1)
    attend(right, 1)
    attend(left, 2)
    for c in range(2 * PIECES):
        output(1, 2, c * PIECE, PIECE)
    low, high = pl.ds(0, HALF), pl.ds(HALF, HALF)
    send(partial.at[1, :, high], left_done.at[:, high], d_s, left_r, to_right)
    send(partial.at[2, :, low], right_done.at[:, low], d_s, right_r, to_left)
    for c in range(PIECES):
        lower = pl.ds(c * PIECE, PIECE)
        higher = pl.ds(HALF + c * PIECE, PIECE)
        received(from_left.at[:, lower], o_r.at[0, c])
        partial[1, :, lower] = (partial[1, :, lower].astype(F32) + from_left[:, lower].astype(F32)).astype(BF16)
        send(partial.at[1, :, lower], left_done.at[:, lower], c_s, left_r, to_right)
        received(from_right.at[:, lower], o_r.at[1, c])
        partial[2, :, higher] = (partial[2, :, higher].astype(F32) + from_right[:, lower].astype(F32)).astype(BF16)
        send(partial.at[2, :, higher], right_done.at[:, higher], c_s, right_r, to_left)
    attend(x, 0)
    for c in range(2 * PIECES):
        output(0, 1, c * PIECE, PIECE)
    received(tg_buf.at[0:7], tg_r)
    for t in range(NT):
        for c in range(4):
            at = t * 512 + c * 128
            mod_rows[4:5, at : at + 128] = tg_buf[t, c : c + 1, :]
    received(left_done, left_r)
    received(right_done, right_r)

    @pl.loop(0, BLOCK // ROWS)
    def _(i):
        at = pl.ds(pl.multiple_of(i * ROWS, ROWS), ROWS)
        projected = partial[0, at, :].astype(F32) + left_done[at, :].astype(F32) + right_done[at, :].astype(F32)
        out[at, :] = (x_raw[x, at, :].astype(F32) + mod_rows[4:5, :] * projected).astype(BF16)

    for copy in drains:
        copy.wait_send()


def shards(
    latent, context, cond, ctx_cond, w_shift, w_scale, w_gate, w_query, key_weight, value_weight, w_out, sink
):
    inverse = (THETA ** (-np.arange(HEAD // 4, dtype=np.float32) * np.float32(2.0) / np.float32(HEAD // 2))).astype(
        np.float32
    )
    inverse = jnp.asarray(np.tile(np.tile(inverse, 4)[None], (8, 1)))
    anywhere = pl.BlockSpec(memory_space=pl.ANY)
    inside = pl.BlockSpec(memory_space=pltpu.VMEM)
    dma = pltpu.SemaphoreType.DMA
    return pl.pallas_call(
        kernel,
        out_shape=pltpu.VMEM((BLOCK, WIDTH), BF16),
        in_specs=[anywhere] * 13,
        out_specs=inside,
        scratch_shapes=[
            pltpu.VMEM((NSP, 128), F32),
            pltpu.VMEM((NSP, 128), F32),
            pltpu.SMEM((16,), F32),
            pltpu.VMEM((8, 128), F32),
            pltpu.VMEM((NX, BLOCK, HEAD), F32),
            pltpu.VMEM((NX, BLOCK, HEAD), F32),
            pltpu.VMEM((NX, BLOCK, WIDTH), BF16),
            pltpu.VMEM((NX, BLOCK, 128), F32),
            pltpu.VMEM((NX, BLOCK, 128), F32),
            pltpu.VMEM((NX * BLOCK, WIDTH), BF16),
            pltpu.VMEM((2, WIDTH, 512), BF16),
            pltpu.VMEM((2, 256, WIDTH), BF16),
            pltpu.VMEM((3, 128, 512), BF16),
            pltpu.VMEM((CTX_ROWS, WIDTH), BF16),
            pltpu.VMEM((CTX_ROWS, WIDTH), BF16),
            pltpu.VMEM((NY, 24, 128), F32),
            pltpu.VMEM((NZ, 16, 128), F32),
            pltpu.VMEM((NT, 16, 128), F32),
            pltpu.VMEM((NZ, 8, 128), F32),
            pltpu.VMEM((NT, 8, 128), F32),
            pltpu.VMEM((8, WIDTH), F32),
            pltpu.VMEM((2, 2, NX * BLOCK, 256), BF16),
            pltpu.VMEM((NX, 4, BLOCK, HEAD), BF16),
            pltpu.VMEM((NX + 2, 2, 4, BLOCK, HEAD), BF16),
            pltpu.VMEM((2, NY, NZ, CTX_ROWS, 256), BF16),
            pltpu.VMEM((2, NX * BLOCK, 2 * HEAD), BF16),
            pltpu.VMEM((NX, BLOCK, WIDTH), BF16),
            pltpu.VMEM((BLOCK, HALF), BF16),
            pltpu.VMEM((BLOCK, HALF), BF16),
            pltpu.VMEM((BLOCK, WIDTH), BF16),
            pltpu.VMEM((BLOCK, WIDTH), BF16),
            dma((13,)), dma((12,)), dma((7,)), dma((8,)), dma((4,)), dma((2, PIECES)), dma((SINGLE,)),
        ],
        compiler_params=pltpu.CompilerParams(
            collective_id=0, has_side_effects=True, vmem_limit_bytes=60 * 1024 * 1024
        ),
    )(
        latent, context, cond.reshape(NSP, 128), ctx_cond.reshape(NSP, 128), w_shift, w_scale, w_gate,
        w_query, key_weight, value_weight, w_out, sink, inverse,
    )


def solution(mesh):
    in_specs = (
        P(("sp", "tp"), None), P("sp", None), P(), P(), P("sp", "tp"), P("sp", "tp"), P("sp", "tp"),
        P(None, "tp"), P(None, "tp"), P(None, "tp"), P("tp", None), P(),
    )
    out_specs = P(("sp", "tp"), None)
    return jax.shard_map(shards, mesh=mesh, in_specs=in_specs, out_specs=out_specs, check_vma=False)
```

```python
import jax
import jax.numpy as jnp
import numpy as np
from jax import lax
from jax.experimental import pallas as pl
from jax.experimental.pallas import tpu as pltpu
from jax.sharding import PartitionSpec as P

MESH = pl.DeviceIdType.MESH
F32 = jnp.float32
BF16 = jnp.bfloat16

NX, NY, NZ, NT = 4, 4, 8, 8
NSP = NY * NZ
HEAD = 128
SIDE = 128
BLOCK = 64
WIDTH = 4096
HALF = WIDTH // 2
PAIR = 2 * BLOCK
TOKENS = 16384
CTX_ROWS = 32
EPS = 1e-05
THETA = 10000.0
MASKED = -1e30
PIECES = 4
PIECE = HALF // PIECES
ROWS = 16
SINGLE = 27


def kernel(
    latent, context, cond_in, ctx_cond_in, w_shift, w_scale, w_gate, wq, wk, wv, wo, sink_in, inverse_in, out,
    conds, sink, inverse, cosines, sines, x_raw, means, scales, x_mod, w_all, w_out, w_modulation, ctx_raw, ctx_mod, y_buf, z_buf, t_buf, zg_buf, tg_buf, mod_rows,
    product, query, kv, ckv, attended, partial, from_left, from_right, left_done, right_done,
    l_sem, ag_r, cy_r, h_r, o_r, c_r, sems,
):
    sp = lax.axis_index("sp")
    tp = lax.axis_index("tp")
    z, y = sp // NY, sp % NY
    x, core = tp // 2, tp % 2
    sibling = x * 2 + 1 - core
    right, opposite, left = (x + 1) % NX, (x + 2) % NX, (x + 3) % NX
    sp_next, sp_back = (sp + 1) % NSP, (sp + NSP - 1) % NSP
    to_right, to_left = (sp, right * 2 + core), (sp, left * 2 + core)
    to_sibling = (sp, sibling)

    def remote(src, dst, send, recv, device):
        return pltpu.make_async_remote_copy(
            src_ref=src, dst_ref=dst, send_sem=send, recv_sem=recv, device_id=device, device_id_type=MESH
        )

    names = iter(range(SINGLE))

    def one():
        return sems.at[next(names)]

    def pair():
        return one(), one()

    def send(*args):
        remote(*args).start()

    def received(ref, sem):
        remote(ref, ref, sem, sem, to_sibling).wait_recv()

    drains = []

    def drained_at_end(ref, sem):
        drains.append(remote(ref, ref, sem, sem, to_sibling))

    local = [
        pltpu.make_async_copy(cond_in, conds.at[0], l_sem.at[0]),
        pltpu.make_async_copy(ctx_cond_in, conds.at[1], l_sem.at[0]),
        pltpu.make_async_copy(w_shift, w_modulation.at[0], l_sem.at[1]),
        pltpu.make_async_copy(w_scale, w_modulation.at[1], l_sem.at[1]),
        pltpu.make_async_copy(w_gate, w_modulation.at[2], l_sem.at[1]),
        pltpu.make_async_copy(latent, x_raw.at[x], l_sem.at[2]),
        pltpu.make_async_copy(context, ctx_raw, l_sem.at[3]),
        pltpu.make_async_copy(sink_in, sink, l_sem.at[4]),
        pltpu.make_async_copy(inverse_in, inverse, l_sem.at[5]),
        pltpu.make_async_copy(wq, w_all.at[core, :, 0:256], l_sem.at[6]),
        pltpu.make_async_copy(wk, w_all.at[core, :, 256:384], l_sem.at[6]),
        pltpu.make_async_copy(wv, w_all.at[core, :, 384:512], l_sem.at[6]),
        pltpu.make_async_copy(wo, w_out.at[core], l_sem.at[7]),
    ]
    for copy in local[:6]:
        copy.start()

    def copied(ref, i):
        pltpu.make_async_copy(ref, ref, l_sem.at[i]).wait()

    barrier = pltpu.get_barrier_semaphore()
    greeted = [(sp, (tp + d) % NT) for d in range(1, NT)]
    greeted += [(z * NY + (y + d) % NY, tp) for d in range(1, NY)]
    greeted += [(((z + d) % NZ) * NY + y, tp) for d in range(1, NZ)]
    greeted += [(sp_next, tp), (sp_next, sibling), (sp_back, tp), (sp_back, sibling)]
    for device in greeted:
        pl.semaphore_signal(barrier, inc=1, device_id=device, device_id_type=MESH)

    copied(conds, 0)
    act = jnp.concatenate(
        [jax.nn.silu(conds[0, pl.ds(sp, 1), :]), jax.nn.silu(conds[1, pl.ds(sp, 1), :]), jnp.zeros((6, 128), F32)],
        axis=0,
    ).astype(BF16)
    y_buf[y] = jnp.zeros((24, 128), F32)
    copied(w_modulation, 1)
    for i in range(3):
        part = jnp.dot(act, w_modulation[i], preferred_element_type=F32)
        for row in range(2 if i < 2 else 1):
            for c in range(4):
                at = (2 * i + row) * 4 + c
                y_buf[y, at : at + 1, :] = part[row : row + 1, c * 128 : (c + 1) * 128]

    pl.semaphore_wait(barrier, len(greeted))

    y_s, y_r = pair()
    for d in range(1, NY):
        send(y_buf.at[y], y_buf.at[y], y_s, y_r, (z * NY + (y + d) % NY, tp))
    drained_at_end(y_buf.at[0:3], y_s)

    local[5].wait()
    ag_s = one()
    drained_at_end(x_raw.at[0:3], ag_s)

    def rows_of(piece):
        return pl.ds(piece * ROWS, ROWS)

    def gather(block, piece, i, device):
        ref = x_raw.at[block, rows_of(piece), :]
        send(ref, ref, ag_s, ag_r.at[i], device)

    def own_pieces(i):
        gather(x, i, min(i, 2), to_right)
        gather(x, 3 - i, 3 + i if i < 2 else 2, to_left)

    def gathered(i):
        received(x_raw.at[left, rows_of(i), :], ag_r.at[i])
        received(x_raw.at[right, rows_of(3 - i), :], ag_r.at[3 + i])

    def forward(i):
        gather(left, i, 5, to_right)
        gather(right, 3 - i, 5, to_left)

    own_pieces(0)
    own_pieces(1)

    for copy in local[6:]:
        copy.start()

    w_s, w_r = pair()
    send(wq, w_all.at[core, :, 0:256], w_s, w_r, to_sibling)
    send(wk, w_all.at[core, :, 256:384], w_s, w_r, to_sibling)
    send(wv, w_all.at[core, :, 384:512], w_s, w_r, to_sibling)
    drained_at_end(w_all.at[core], w_s)

    def moments(read, rows):
        chunks = [slice(i * 128, (i + 1) * 128) for i in range(WIDTH // 128)]
        mean = jnp.sum(sum(read(at).astype(F32) for at in chunks), axis=-1, keepdims=True) / WIDTH
        mean = jnp.broadcast_to(mean, (rows, 128))
        var = sum(jnp.square(read(at).astype(F32) - mean) for at in chunks)
        var = jnp.sum(var, axis=-1, keepdims=True) / WIDTH
        return mean, jnp.broadcast_to(lax.rsqrt(var + EPS), (rows, 128))

    def statistics(block, half):
        rows = slice(half * 32, half * 32 + 32)
        means[block, rows, :], scales[block, rows, :] = moments(lambda at: x_raw[block, rows, at], 32)

    @pl.loop(0, 2)
    def _(i):
        at = pl.ds(pl.multiple_of(i * 32, 32), 32)
        means[x, at, :], scales[x, at, :] = moments(lambda columns: x_raw[x, at, columns], 32)

    lane = lax.broadcasted_iota(jnp.int32, (BLOCK, HEAD), 1)
    column = lax.broadcasted_iota(jnp.int32, (BLOCK, HEAD), 0)
    by_row = lane < HEAD // 2
    is_first = lane % (HEAD // 2) < HEAD // 4

    local[7].wait()
    local[8].wait()

    @pl.loop(0, NX)
    def _(b):
        position = jnp.where(by_row, sp * NT + b * 2 + core, column).astype(F32)
        angle = position * inverse[0:1, :]
        cosines[b] = jnp.cos(angle)
        sine = jnp.sin(angle)
        sines[b] = jnp.where(is_first, -sine, sine)

    received(y_buf.at[0:3], y_r)
    total = jnp.sum(y_buf[...], axis=0)
    z_buf[z] = total[0:16]
    zg_buf[z] = total[16:24]
    z_s, z_r = pair()
    for d in (4, 3, 5, 2, 6, 1, 7):
        send(z_buf.at[z], z_buf.at[z], z_s, z_r, (((z + d) % NZ) * NY + y, tp))
    drained_at_end(z_buf.at[0:7], z_s)
    own_pieces(2)
    received(z_buf.at[0:7], z_r)
    t_buf[tp] = jnp.sum(z_buf[...], axis=0)
    t_s, t_r = pair()
    for d in (4, 5, 3, 2, 6, 7, 1):
        send(t_buf.at[tp], t_buf.at[tp], t_s, t_r, (sp, (tp + d) % NT))
    drained_at_end(t_buf.at[0:7], t_s)
    own_pieces(3)
    zg_s, zg_r = pair()
    for d in range(1, NZ):
        send(zg_buf.at[z], zg_buf.at[z], zg_s, zg_r, (((z + d) % NZ) * NY + y, tp))
    drained_at_end(zg_buf.at[0:7], zg_s)
    wo_s, wo_r = pair()
    send(wo, w_out.at[core], wo_s, wo_r, to_sibling)
    drained_at_end(w_out.at[core], wo_s)

    for i in range(2):
        gathered(i)
        forward(i)

    statistics(left, 0)
    statistics(right, 1)
    local[6].wait()
    ctx_mean, ctx_scale = moments(lambda at: ctx_raw[:, at], CTX_ROWS)

    received(t_buf.at[0:7], t_r)
    for t in range(NT):
        values = t_buf[t]
        for row in range(4):
            for c in range(4):
                at = t * 512 + c * 128
                value = values[row * 4 + c : row * 4 + c + 1, :]
                mod_rows[row : row + 1, at : at + 128] = 1.0 + value if row > 1 else value

    for i in range(WIDTH // 128):
        at = slice(i * 128, (i + 1) * 128)
        normal = (ctx_raw[:, at].astype(F32) - ctx_mean) * ctx_scale
        ctx_mod[:, at] = (normal * mod_rows[3:4, at] + mod_rows[1:2, at]).astype(BF16)
    copied(w_all.at[core], 6)
    local[12].wait()
    halves = [
        jnp.dot(ctx_mod[:, at], w_all[core, at, 256:512], preferred_element_type=F32)
        for at in (slice(0, HALF), slice(HALF, WIDTH))
    ]
    ckv[core, y, z] = (halves[0] + halves[1]).astype(BF16)

    cz_s, cz_r = pair()
    ctx_s, cc_r = pair()

    near_z = (1, 7, 2, 6)

    def spread(d):
        line = ckv.at[core, y, (z + NZ - d) % NZ]
        if d not in near_z:
            for e in (2, 1, 3):
                send(line, line, ctx_s, cy_r.at[min(d, 1)], (z * NY + (y + e) % NY, tp))
        send(line, line, ctx_s, cc_r, to_sibling)

    def relay(d):
        there = (z + NZ - d) % NZ
        for e in range(1, NY):
            line = ckv.at[core, (y + NY - e) % NY, there]
            if d == 0:
                for f in near_z:
                    send(line, line, ctx_s, cy_r.at[2], (((z + f) % NZ) * NY + y, tp))
            send(line, line, ctx_s, cc_r, to_sibling)

    own = ckv.at[core, y, z]
    for d in (4, 3, 5, 2, 6, 1, 7):
        send(own, own, cz_s, cz_r, (((z + d) % NZ) * NY + y, tp))
    drained_at_end(ckv.at[core, 0, 0:7], cz_s)
    drained_at_end(ckv.at[0:2, 0:4, 0:7], ctx_s)
    spread(0)

    blocks = (x, right, left, opposite)

    def modulate(slot):
        block = blocks[slot]

        @pl.loop(0, WIDTH // 512)
        def _(c):
            for q in range(4):
                at = pl.ds(pl.multiple_of(c * 512 + q * 128, 128), 128)
                normal = (x_raw[block, :, at].astype(F32) - means[block]) * scales[block]
                x_mod[slot * BLOCK : (slot + 1) * BLOCK, at] = (
                    normal * mod_rows[2:3, at] + mod_rows[0:1, at]
                ).astype(BF16)

    modulate(0)
    received(x_raw.at[left], ag_r.at[2])

    statistics(left, 1)
    statistics(right, 0)

    modulate(1)
    modulate(2)

    def project(c, slot, slots):
        rows = slice(slot * BLOCK, (slot + slots) * BLOCK)
        for j in range(2):
            product[j, c, rows, :] = jnp.dot(
                x_mod[rows, :], w_all[j, :, c * 256 : (c + 1) * 256], preferred_element_type=F32
            ).astype(BF16)

    def place(slot):
        return (x + slot + slot // 2 * (5 - 2 * slot)) % NX, pl.ds(pl.multiple_of(slot * BLOCK, BLOCK), BLOCK)

    def turned(value, b):
        value = value.astype(F32)
        partner = jnp.where(is_first, pltpu.roll(value, 96, 1), pltpu.roll(value, 32, 1))
        return (value * cosines[b] + partner * sines[b]).astype(BF16)

    def turn_keys(slot):
        b, rows = place(slot)
        for j in range(2):
            kv[b + 1, core, j] = turned(product[j, 1, rows, 0:HEAD], b)
            kv[b + 1, core, 2 + j] = product[j, 1, rows, HEAD : 2 * HEAD]

    def turn_queries(slot):
        b, rows = place(slot)
        for j in range(2):
            for g in range(2):
                query[b, 2 * j + g] = turned(product[j, 0, rows, g * HEAD : (g + 1) * HEAD], b)

    kv_s, kv_r = pair()
    drained_at_end(kv.at[1:5, core], kv_s)

    def share(slot):
        ref = kv.at[blocks[slot] + 1, core]
        send(ref, ref, kv_s, kv_r, to_sibling)

    h_s = one()
    drained_at_end(kv.at[1:4, core], h_s)
    to_next = remote(kv.at[NX, core], kv.at[0, core], h_s, h_r.at[0], (sp_next, tp))
    to_back = remote(kv.at[1, core], kv.at[NX + 1, core], h_s, h_r.at[2], (sp_back, tp))
    to_next_other = remote(kv.at[NX, core], kv.at[0, core], h_s, h_r.at[1], (sp_next, sibling))
    to_back_other = remote(kv.at[1, core], kv.at[NX + 1, core], h_s, h_r.at[3], (sp_back, sibling))
    kv[(NX + 1) * (1 - core), 1 - core] = jnp.zeros((4, BLOCK, HEAD), BF16)

    def halo_when(last, first):
        @pl.when(last)
        def _():
            to_next.start()

            @pl.when(core == 1)
            def _():
                to_next_other.start()

        @pl.when(first)
        def _():
            to_back.start()

            @pl.when(core == 0)
            def _():
                to_back_other.start()

    def halo_received(first, last):
        @pl.when(first)
        def _():
            received(kv.at[0, core], h_r.at[0])

            @pl.when(core == 0)
            def _():
                received(kv.at[0, 1], h_r.at[1])

        @pl.when(last)
        def _():
            received(kv.at[NX + 1, core], h_r.at[2])

            @pl.when(core == 1)
            def _():
                received(kv.at[NX + 1, 0], h_r.at[3])

    other = w_all.at[1 - core]
    received(other, w_r)
    project(1, 0, 3)
    received(ckv.at[core, 0:3, 0], cy_r.at[0])
    relay(0)

    @pl.loop(0, 3)
    def _(slot):
        turn_keys(slot)

    for slot in range(3):
        share(slot)
    halo_when(opposite != NX - 1, opposite != 0)
    project(0, 0, 3)

    received(ckv.at[core, 0, 0:7], cz_r)
    for d in (3, 5, 4, 1, 7, 2, 6):
        spread(d)
    @pl.loop(0, 3)
    def _(slot):
        turn_queries(slot)

    received(x_raw.at[opposite], ag_r.at[5])

    received(zg_buf.at[0:7], zg_r)
    tg_buf[tp] = jnp.sum(zg_buf[...], axis=0)
    tg_s, tg_r = pair()
    for d in range(1, NT):
        send(tg_buf.at[tp], tg_buf.at[tp], tg_s, tg_r, (sp, (tp + d) % NT))
    drained_at_end(tg_buf.at[0:7], tg_s)

    statistics(opposite, 0)
    statistics(opposite, 1)
    modulate(3)
    project(1, 3, 1)
    turn_keys(3)
    share(3)
    halo_when(opposite == NX - 1, opposite == 0)
    project(0, 3, 1)
    turn_queries(3)
    received(ckv.at[core, 0:3, 0:4], cy_r.at[2])
    for d in (1, 7, 2, 6):
        relay(d)
    received(ckv.at[core, 0:3, 0:3], cy_r.at[1])
    for d in (3, 5, 4):
        relay(d)
    received(kv.at[1:5, 1 - core], kv_r)
    halo_received(opposite == 0, opposite == NX - 1)

    power = HEAD ** (-0.5) * np.log2(np.e).item()
    to_scores = HEAD**0.5
    i_query = lax.broadcasted_iota(jnp.int32, (PAIR, 3 * PAIR), 0) % BLOCK + core * BLOCK
    i_key = lax.broadcasted_iota(jnp.int32, (PAIR, 3 * PAIR), 1) - PAIR
    near = jnp.abs(i_key - i_query) <= SIDE
    upper = lax.broadcasted_iota(jnp.int32, (PAIR, 1), 0) < BLOCK
    across = (((1,), (1,)), ((), ()))

    def attend(b, slot, heads=(0, 1)):
        key_at = i_key + (sp * NT * BLOCK + b * PAIR)
        valid = near & (key_at >= 0) & (key_at < TOKENS)
        for h in heads:
            q = query[b, pl.ds(2 * h, 2)].reshape(PAIR, HEAD)
            k_band = kv[pl.ds(b, 3), :, h].reshape(3 * PAIR, HEAD)
            v_band = kv[pl.ds(b, 3), :, 2 + h].reshape(3 * PAIR, HEAD)
            k_ctx = ckv[h, :, :, :, 0:HEAD].reshape(NSP * CTX_ROWS, HEAD)
            v_ctx = ckv[h, :, :, :, HEAD : 2 * HEAD].reshape(NSP * CTX_ROWS, HEAD)
            s_band = lax.dot_general(q, k_band, across, preferred_element_type=F32)
            s_band = jnp.where(valid, s_band, MASKED)
            s_ctx = lax.dot_general(q, k_ctx, across, preferred_element_type=F32)
            sinks = jnp.where(upper, sink[4 * x + 2 * h], sink[4 * x + 2 * h + 1]) * to_scores
            top = jnp.maximum(
                jnp.maximum(jnp.max(s_band, axis=-1, keepdims=True), jnp.max(s_ctx, axis=-1, keepdims=True)), sinks
            )
            e_band = jnp.exp2((s_band - top) * power)
            e_ctx = jnp.exp2((s_ctx - top) * power)
            total = (
                jnp.sum(e_band, axis=-1, keepdims=True)
                + jnp.sum(e_ctx, axis=-1, keepdims=True)
                + jnp.exp2((sinks - top) * power)
            )
            value = jnp.dot(e_band.astype(BF16), v_band, preferred_element_type=F32)
            value += jnp.dot(e_ctx.astype(BF16), v_ctx, preferred_element_type=F32)
            value = (value / total).astype(BF16)
            rows = slice(slot * BLOCK, (slot + 1) * BLOCK)
            for g in range(2):
                attended[h, rows, g * HEAD : (g + 1) * HEAD] = value[g * BLOCK : (g + 1) * BLOCK]

    def output(slot, slots, at, width):
        rows = slice(slot * BLOCK, (slot + slots) * BLOCK)
        columns = slice(at, at + width)
        result = jnp.dot(attended[0, rows, :], w_out[0, :, columns], preferred_element_type=F32)
        result += jnp.dot(attended[1, rows, :], w_out[1, :, columns], preferred_element_type=F32)
        result = result.astype(BF16)
        for s in range(slots):
            partial[slot + s, :, columns] = result[s * BLOCK : (s + 1) * BLOCK]

    attend(opposite, 3, (core,))
    received(ckv.at[1 - core], cc_r)
    attend(opposite, 3, (1 - core,))
    received(w_out.at[1 - core], wo_r)
    ring_s = one()
    left_r, right_r = pair()
    drained_at_end(partial.at[0:3], ring_s)
    for c in range(PIECES):
        output(3, 1, c * PIECE, PIECE)
        output(3, 1, HALF + c * PIECE, PIECE)
        lower = pl.ds(c * PIECE, PIECE)
        higher = pl.ds(HALF + c * PIECE, PIECE)
        send(partial.at[3, :, lower], from_left.at[:, lower], ring_s, o_r.at[0, c], to_right)
        send(partial.at[3, :, higher], from_right.at[:, lower], ring_s, o_r.at[1, c], to_left)
    halo_received(opposite != 0, opposite != NX - 1)
    attend(right, 1)
    attend(left, 2)
    for c in range(2 * PIECES):
        output(1, 2, c * PIECE, PIECE)
    low, high = pl.ds(0, HALF), pl.ds(HALF, HALF)
    send(partial.at[1, :, high], left_done.at[:, high], ring_s, left_r, to_right)
    send(partial.at[2, :, low], right_done.at[:, low], ring_s, right_r, to_left)
    for c in range(PIECES):
        lower = pl.ds(c * PIECE, PIECE)
        higher = pl.ds(HALF + c * PIECE, PIECE)
        received(from_left.at[:, lower], o_r.at[0, c])
        partial[1, :, lower] = (partial[1, :, lower].astype(F32) + from_left[:, lower].astype(F32)).astype(BF16)
        send(partial.at[1, :, lower], left_done.at[:, lower], ring_s, c_r.at[0, c], to_right)
        received(from_right.at[:, lower], o_r.at[1, c])
        partial[2, :, higher] = (partial[2, :, higher].astype(F32) + from_right[:, lower].astype(F32)).astype(BF16)
        send(partial.at[2, :, higher], right_done.at[:, higher], ring_s, c_r.at[1, c], to_left)
    attend(x, 0)
    for c in range(2 * PIECES):
        output(0, 1, c * PIECE, PIECE)
    received(tg_buf.at[0:7], tg_r)
    for t in range(NT):
        for c in range(4):
            at = t * 512 + c * 128
            mod_rows[4:5, at : at + 128] = tg_buf[t, c : c + 1, :]
    received(left_done.at[:, high], left_r)
    received(right_done.at[:, low], right_r)
    for c in range(PIECES):
        for half, done in enumerate((left_done, right_done)):
            at = pl.ds(half * HALF + c * PIECE, PIECE)
            received(done.at[:, at], c_r.at[half, c])
            projected = partial[0, :, at].astype(F32) + left_done[:, at].astype(F32) + right_done[:, at].astype(F32)
            out[:, at] = (x_raw[x, :, at].astype(F32) + mod_rows[4:5, at] * projected).astype(BF16)

    for copy in drains:
        copy.wait_send()


def shards(
    latent, context, cond, ctx_cond, w_shift, w_scale, w_gate, w_query, key_weight, value_weight, w_out, sink
):
    inverse = (THETA ** (-np.arange(HEAD // 4, dtype=np.float32) * np.float32(2.0) / np.float32(HEAD // 2))).astype(
        np.float32
    )
    inverse = jnp.asarray(np.tile(np.tile(inverse, 4)[None], (8, 1)))
    anywhere = pl.BlockSpec(memory_space=pl.ANY)
    inside = pl.BlockSpec(memory_space=pltpu.VMEM)
    dma = pltpu.SemaphoreType.DMA
    return pl.pallas_call(
        kernel,
        out_shape=pltpu.VMEM((BLOCK, WIDTH), BF16),
        in_specs=[anywhere] * 13,
        out_specs=inside,
        scratch_shapes=[
            pltpu.VMEM((2, NSP, 128), F32),
            pltpu.SMEM((16,), F32),
            pltpu.VMEM((8, 128), F32),
            pltpu.VMEM((NX, BLOCK, HEAD), F32),
            pltpu.VMEM((NX, BLOCK, HEAD), F32),
            pltpu.VMEM((NX, BLOCK, WIDTH), BF16),
            pltpu.VMEM((NX, BLOCK, 128), F32),
            pltpu.VMEM((NX, BLOCK, 128), F32),
            pltpu.VMEM((NX * BLOCK, WIDTH), BF16),
            pltpu.VMEM((2, WIDTH, 512), BF16),
            pltpu.VMEM((2, 256, WIDTH), BF16),
            pltpu.VMEM((3, 128, 512), BF16),
            pltpu.VMEM((CTX_ROWS, WIDTH), BF16),
            pltpu.VMEM((CTX_ROWS, WIDTH), BF16),
            pltpu.VMEM((NY, 24, 128), F32),
            pltpu.VMEM((NZ, 16, 128), F32),
            pltpu.VMEM((NT, 16, 128), F32),
            pltpu.VMEM((NZ, 8, 128), F32),
            pltpu.VMEM((NT, 8, 128), F32),
            pltpu.VMEM((8, WIDTH), F32),
            pltpu.VMEM((2, 2, NX * BLOCK, 256), BF16),
            pltpu.VMEM((NX, 4, BLOCK, HEAD), BF16),
            pltpu.VMEM((NX + 2, 2, 4, BLOCK, HEAD), BF16),
            pltpu.VMEM((2, NY, NZ, CTX_ROWS, 256), BF16),
            pltpu.VMEM((2, NX * BLOCK, 2 * HEAD), BF16),
            pltpu.VMEM((NX, BLOCK, WIDTH), BF16),
            pltpu.VMEM((BLOCK, HALF), BF16),
            pltpu.VMEM((BLOCK, HALF), BF16),
            pltpu.VMEM((BLOCK, WIDTH), BF16),
            pltpu.VMEM((BLOCK, WIDTH), BF16),
            dma((8,)), dma((6,)), dma((3,)), dma((4,)), dma((2, PIECES)), dma((2, PIECES)), dma((SINGLE,)),
        ],
        compiler_params=pltpu.CompilerParams(
            collective_id=0, has_side_effects=True, vmem_limit_bytes=60 * 1024 * 1024
        ),
    )(
        latent, context, cond.reshape(NSP, 128), ctx_cond.reshape(NSP, 128), w_shift, w_scale, w_gate,
        w_query, key_weight, value_weight, w_out, sink, inverse,
    )


def solution(mesh):
    in_specs = (
        P(("sp", "tp"), None), P("sp", None), P(), P(), P("sp", "tp"), P("sp", "tp"), P("sp", "tp"),
        P(None, "tp"), P(None, "tp"), P(None, "tp"), P("tp", None), P(),
    )
    out_specs = P(("sp", "tp"), None)
    return jax.shard_map(shards, mesh=mesh, in_specs=in_specs, out_specs=out_specs, check_vma=False)
```

```python
import jax
import jax.numpy as jnp
import numpy as np
from jax import lax
from jax.experimental import pallas as pl
from jax.experimental.pallas import tpu as pltpu
from jax.sharding import PartitionSpec as P

MESH = pl.DeviceIdType.MESH
F32 = jnp.float32
BF16 = jnp.bfloat16

NX, NY, NZ, NT = 4, 4, 8, 8
NSP = NY * NZ
HEAD = 128
SIDE = 128
BLOCK = 64
WIDTH = 4096
HALF = WIDTH // 2
PAIR = 2 * BLOCK
TOKENS = 16384
CTX_ROWS = 32
EPS = 1e-05
THETA = 10000.0
MASKED = -1e30
PIECES = 4
PIECE = HALF // PIECES
ROWS = 16
SINGLE = 27


def kernel(
    latent, context, cond_in, ctx_cond_in, w_shift, w_scale, w_gate, wq, wk, wv, wo, sink_in, inverse_in, out,
    conds, sink, inverse, cosines, sines, x_raw, means, scales, x_mod, w_all, w_out, w_modulation, ctx_raw, ctx_mod, y_buf, z_buf, t_buf, zg_buf, tg_buf, mod_rows,
    product, query, kv, ckv, attended, partial, from_left, from_right, left_done, right_done,
    l_sem, ag_r, cy_r, h_r, o_r, c_r, sems,
):
    sp = lax.axis_index("sp")
    tp = lax.axis_index("tp")
    z, y = sp // NY, sp % NY
    x, core = tp // 2, tp % 2
    sibling = x * 2 + 1 - core
    right, opposite, left = (x + 1) % NX, (x + 2) % NX, (x + 3) % NX
    sp_next, sp_back = (sp + 1) % NSP, (sp + NSP - 1) % NSP
    to_right, to_left = (sp, right * 2 + core), (sp, left * 2 + core)
    to_sibling = (sp, sibling)

    def remote(src, dst, send, recv, device):
        return pltpu.make_async_remote_copy(
            src_ref=src, dst_ref=dst, send_sem=send, recv_sem=recv, device_id=device, device_id_type=MESH
        )

    names = iter(range(SINGLE))

    def one():
        return sems.at[next(names)]

    def pair():
        return one(), one()

    def send(*args):
        remote(*args).start()

    def received(ref, sem):
        remote(ref, ref, sem, sem, to_sibling).wait_recv()

    drains = []

    def drained_at_end(ref, sem):
        drains.append(remote(ref, ref, sem, sem, to_sibling))

    local = [
        pltpu.make_async_copy(cond_in, conds.at[0], l_sem.at[0]),
        pltpu.make_async_copy(ctx_cond_in, conds.at[1], l_sem.at[0]),
        pltpu.make_async_copy(w_shift, w_modulation.at[0], l_sem.at[1]),
        pltpu.make_async_copy(w_scale, w_modulation.at[1], l_sem.at[1]),
        pltpu.make_async_copy(w_gate, w_modulation.at[2], l_sem.at[1]),
        pltpu.make_async_copy(latent, x_raw.at[x], l_sem.at[2]),
        pltpu.make_async_copy(context, ctx_raw, l_sem.at[3]),
        pltpu.make_async_copy(sink_in, sink, l_sem.at[4]),
        pltpu.make_async_copy(inverse_in, inverse, l_sem.at[5]),
        pltpu.make_async_copy(wq, w_all.at[core, :, 0:256], l_sem.at[6]),
        pltpu.make_async_copy(wk, w_all.at[core, :, 256:384], l_sem.at[6]),
        pltpu.make_async_copy(wv, w_all.at[core, :, 384:512], l_sem.at[6]),
        pltpu.make_async_copy(wo, w_out.at[core], l_sem.at[7]),
    ]
    for copy in local[:6]:
        copy.start()

    def copied(ref, i):
        pltpu.make_async_copy(ref, ref, l_sem.at[i]).wait()

    barrier = pltpu.get_barrier_semaphore()
    greeted = [(sp, (tp + d) % NT) for d in range(1, NT)]
    greeted += [(z * NY + (y + d) % NY, tp) for d in range(1, NY)]
    greeted += [(((z + d) % NZ) * NY + y, tp) for d in range(1, NZ)]
    greeted += [(sp_next, tp), (sp_next, sibling), (sp_back, tp), (sp_back, sibling)]
    for device in greeted:
        pl.semaphore_signal(barrier, inc=1, device_id=device, device_id_type=MESH)

    copied(conds, 0)
    act = jnp.concatenate(
        [jax.nn.silu(conds[0, pl.ds(sp, 1), :]), jax.nn.silu(conds[1, pl.ds(sp, 1), :]), jnp.zeros((6, 128), F32)],
        axis=0,
    ).astype(BF16)
    y_buf[y] = jnp.zeros((24, 128), F32)
    copied(w_modulation, 1)
    for i in range(3):
        part = jnp.dot(act, w_modulation[i], preferred_element_type=F32)
        for row in range(2 if i < 2 else 1):
            for c in range(4):
                at = (2 * i + row) * 4 + c
                y_buf[y, at : at + 1, :] = part[row : row + 1, c * 128 : (c + 1) * 128]

    pl.semaphore_wait(barrier, len(greeted))

    y_s, y_r = pair()
    for d in range(1, NY):
        send(y_buf.at[y], y_buf.at[y], y_s, y_r, (z * NY + (y + d) % NY, tp))
    drained_at_end(y_buf.at[0:3], y_s)

    local[5].wait()
    ag_s = one()
    drained_at_end(x_raw.at[0:3], ag_s)

    def rows_of(piece):
        return pl.ds(piece * ROWS, ROWS)

    def gather(block, piece, i, device):
        ref = x_raw.at[block, rows_of(piece), :]
        send(ref, ref, ag_s, ag_r.at[i], device)

    def own_pieces(i):
        gather(x, i, min(i, 2), to_right)
        gather(x, 3 - i, 3 + i if i < 2 else 2, to_left)

    def gathered(i):
        received(x_raw.at[left, rows_of(i), :], ag_r.at[i])
        received(x_raw.at[right, rows_of(3 - i), :], ag_r.at[3 + i])

    def forward(i):
        gather(left, i, 5, to_right)
        gather(right, 3 - i, 5, to_left)

    own_pieces(0)
    own_pieces(1)

    for copy in local[6:]:
        copy.start()

    w_s, w_r = pair()
    send(wq, w_all.at[core, :, 0:256], w_s, w_r, to_sibling)
    send(wk, w_all.at[core, :, 256:384], w_s, w_r, to_sibling)
    send(wv, w_all.at[core, :, 384:512], w_s, w_r, to_sibling)
    drained_at_end(w_all.at[core], w_s)

    def moments(read, rows):
        chunks = [slice(i * 128, (i + 1) * 128) for i in range(WIDTH // 128)]
        mean = jnp.sum(sum(read(at).astype(F32) for at in chunks), axis=-1, keepdims=True) / WIDTH
        mean = jnp.broadcast_to(mean, (rows, 128))
        var = sum(jnp.square(read(at).astype(F32) - mean) for at in chunks)
        var = jnp.sum(var, axis=-1, keepdims=True) / WIDTH
        return mean, jnp.broadcast_to(lax.rsqrt(var + EPS), (rows, 128))

    def statistics(block, half):
        rows = slice(half * 32, half * 32 + 32)
        means[block, rows, :], scales[block, rows, :] = moments(lambda at: x_raw[block, rows, at], 32)

    @pl.loop(0, 2)
    def _(i):
        at = pl.ds(pl.multiple_of(i * 32, 32), 32)
        means[x, at, :], scales[x, at, :] = moments(lambda columns: x_raw[x, at, columns], 32)

    lane = lax.broadcasted_iota(jnp.int32, (BLOCK, HEAD), 1)
    column = lax.broadcasted_iota(jnp.int32, (BLOCK, HEAD), 0)
    by_row = lane < HEAD // 2
    is_first = lane % (HEAD // 2) < HEAD // 4

    local[7].wait()
    local[8].wait()

    @pl.loop(0, NX)
    def _(b):
        position = jnp.where(by_row, sp * NT + b * 2 + core, column).astype(F32)
        angle = position * inverse[0:1, :]
        cosines[b] = jnp.cos(angle)
        sine = jnp.sin(angle)
        sines[b] = jnp.where(is_first, -sine, sine)

    received(y_buf.at[0:3], y_r)
    total = jnp.sum(y_buf[...], axis=0)
    z_buf[z] = total[0:16]
    zg_buf[z] = total[16:24]
    z_s, z_r = pair()
    for d in (4, 3, 5, 2, 6, 1, 7):
        send(z_buf.at[z], z_buf.at[z], z_s, z_r, (((z + d) % NZ) * NY + y, tp))
    drained_at_end(z_buf.at[0:7], z_s)
    own_pieces(2)
    received(z_buf.at[0:7], z_r)
    t_buf[tp] = jnp.sum(z_buf[...], axis=0)
    t_s, t_r = pair()
    for d in (4, 5, 3, 2, 6, 7, 1):
        send(t_buf.at[tp], t_buf.at[tp], t_s, t_r, (sp, (tp + d) % NT))
    drained_at_end(t_buf.at[0:7], t_s)
    own_pieces(3)
    zg_s, zg_r = pair()
    for d in range(1, NZ):
        send(zg_buf.at[z], zg_buf.at[z], zg_s, zg_r, (((z + d) % NZ) * NY + y, tp))
    drained_at_end(zg_buf.at[0:7], zg_s)
    wo_s, wo_r = pair()
    send(wo, w_out.at[core], wo_s, wo_r, to_sibling)
    drained_at_end(w_out.at[core], wo_s)

    for i in range(2):
        gathered(i)
        forward(i)

    statistics(left, 0)
    statistics(right, 1)
    local[6].wait()
    ctx_mean, ctx_scale = moments(lambda at: ctx_raw[:, at], CTX_ROWS)

    received(t_buf.at[0:7], t_r)
    for t in range(NT):
        values = t_buf[t]
        for row in range(4):
            for c in range(4):
                at = t * 512 + c * 128
                value = values[row * 4 + c : row * 4 + c + 1, :]
                mod_rows[row : row + 1, at : at + 128] = 1.0 + value if row > 1 else value

    for i in range(WIDTH // 128):
        at = slice(i * 128, (i + 1) * 128)
        normal = (ctx_raw[:, at].astype(F32) - ctx_mean) * ctx_scale
        ctx_mod[:, at] = (normal * mod_rows[3:4, at] + mod_rows[1:2, at]).astype(BF16)
    copied(w_all.at[core], 6)
    local[12].wait()
    halves = [
        jnp.dot(ctx_mod[:, at], w_all[core, at, 256:512], preferred_element_type=F32)
        for at in (slice(0, HALF), slice(HALF, WIDTH))
    ]
    ckv[core, y, z] = (halves[0] + halves[1]).astype(BF16)

    cz_s, cz_r = pair()
    ctx_s, cc_r = pair()

    near_z = (1, 7, 2, 6)

    def spread(d):
        line = ckv.at[core, y, (z + NZ - d) % NZ]
        if d not in near_z:
            for e in (2, 1, 3):
                send(line, line, ctx_s, cy_r.at[min(d, 1)], (z * NY + (y + e) % NY, tp))
        send(line, line, ctx_s, cc_r, to_sibling)

    def relay(d):
        there = (z + NZ - d) % NZ
        for e in range(1, NY):
            line = ckv.at[core, (y + NY - e) % NY, there]
            if d == 0:
                for f in near_z:
                    send(line, line, ctx_s, cy_r.at[2], (((z + f) % NZ) * NY + y, tp))
            send(line, line, ctx_s, cc_r, to_sibling)

    own = ckv.at[core, y, z]
    for d in (4, 3, 5, 2, 6, 1, 7):
        send(own, own, cz_s, cz_r, (((z + d) % NZ) * NY + y, tp))
    drained_at_end(ckv.at[core, 0, 0:7], cz_s)
    drained_at_end(ckv.at[0:2, 0:4, 0:7], ctx_s)
    spread(0)

    blocks = (x, right, left, opposite)

    def modulate(slot):
        block = blocks[slot]

        @pl.loop(0, WIDTH // 512)
        def _(c):
            for q in range(4):
                at = pl.ds(pl.multiple_of(c * 512 + q * 128, 128), 128)
                normal = (x_raw[block, :, at].astype(F32) - means[block]) * scales[block]
                x_mod[slot * BLOCK : (slot + 1) * BLOCK, at] = (
                    normal * mod_rows[2:3, at] + mod_rows[0:1, at]
                ).astype(BF16)

    modulate(0)
    received(x_raw.at[left], ag_r.at[2])

    statistics(left, 1)
    statistics(right, 0)

    modulate(1)
    modulate(2)

    def project(c, slot, slots):
        rows = slice(slot * BLOCK, (slot + slots) * BLOCK)
        for j in range(2):
            product[j, c, rows, :] = jnp.dot(
                x_mod[rows, :], w_all[j, :, c * 256 : (c + 1) * 256], preferred_element_type=F32
            ).astype(BF16)

    def place(slot):
        return (x + slot + slot // 2 * (5 - 2 * slot)) % NX, pl.ds(pl.multiple_of(slot * BLOCK, BLOCK), BLOCK)

    def turned(value, b):
        value = value.astype(F32)
        partner = jnp.where(is_first, pltpu.roll(value, 96, 1), pltpu.roll(value, 32, 1))
        return (value * cosines[b] + partner * sines[b]).astype(BF16)

    def turn_keys(slot):
        b, rows = place(slot)
        for j in range(2):
            kv[b + 1, core, j] = turned(product[j, 1, rows, 0:HEAD], b)
            kv[b + 1, core, 2 + j] = product[j, 1, rows, HEAD : 2 * HEAD]

    def turn_queries(slot):
        b, rows = place(slot)
        for j in range(2):
            for g in range(2):
                query[b, 2 * j + g] = turned(product[j, 0, rows, g * HEAD : (g + 1) * HEAD], b)

    kv_s, kv_r = pair()
    drained_at_end(kv.at[1:5, core], kv_s)

    def share(slot):
        ref = kv.at[blocks[slot] + 1, core]
        send(ref, ref, kv_s, kv_r, to_sibling)

    h_s = one()
    drained_at_end(kv.at[1:4, core], h_s)
    to_next = remote(kv.at[NX, core], kv.at[0, core], h_s, h_r.at[0], (sp_next, tp))
    to_back = remote(kv.at[1, core], kv.at[NX + 1, core], h_s, h_r.at[2], (sp_back, tp))
    to_next_other = remote(kv.at[NX, core], kv.at[0, core], h_s, h_r.at[1], (sp_next, sibling))
    to_back_other = remote(kv.at[1, core], kv.at[NX + 1, core], h_s, h_r.at[3], (sp_back, sibling))
    kv[(NX + 1) * (1 - core), 1 - core] = jnp.zeros((4, BLOCK, HEAD), BF16)

    def halo_when(last, first):
        @pl.when(last)
        def _():
            to_next.start()

            @pl.when(core == 1)
            def _():
                to_next_other.start()

        @pl.when(first)
        def _():
            to_back.start()

            @pl.when(core == 0)
            def _():
                to_back_other.start()

    def halo_received(first, last):
        @pl.when(first)
        def _():
            received(kv.at[0, core], h_r.at[0])

            @pl.when(core == 0)
            def _():
                received(kv.at[0, 1], h_r.at[1])

        @pl.when(last)
        def _():
            received(kv.at[NX + 1, core], h_r.at[2])

            @pl.when(core == 1)
            def _():
                received(kv.at[NX + 1, 0], h_r.at[3])

    other = w_all.at[1 - core]
    received(other, w_r)
    project(1, 0, 3)
    received(ckv.at[core, 0:3, 0], cy_r.at[0])
    relay(0)

    @pl.loop(0, 3)
    def _(slot):
        turn_keys(slot)

    for slot in range(3):
        share(slot)
    halo_when(x == 2, x == 1)
    project(0, 0, 3)

    received(ckv.at[core, 0, 0:7], cz_r)
    for d in (3, 5, 4, 1, 7, 2, 6):
        spread(d)
    halo_when((x == 0) | (x == NX - 1), (x == 0) | (x == NX - 1))
    @pl.loop(0, 3)
    def _(slot):
        turn_queries(slot)

    received(x_raw.at[opposite], ag_r.at[5])

    received(zg_buf.at[0:7], zg_r)
    tg_buf[tp] = jnp.sum(zg_buf[...], axis=0)
    tg_s, tg_r = pair()
    for d in range(1, NT):
        send(tg_buf.at[tp], tg_buf.at[tp], tg_s, tg_r, (sp, (tp + d) % NT))
    drained_at_end(tg_buf.at[0:7], tg_s)

    statistics(opposite, 0)
    statistics(opposite, 1)
    modulate(3)
    project(1, 3, 1)
    turn_keys(3)
    share(3)
    halo_when(opposite == NX - 1, opposite == 0)
    project(0, 3, 1)
    turn_queries(3)
    received(ckv.at[core, 0:3, 0:4], cy_r.at[2])
    for d in (1, 7, 2, 6):
        relay(d)
    received(ckv.at[core, 0:3, 0:3], cy_r.at[1])
    for d in (3, 5, 4):
        relay(d)
    received(kv.at[1:5, 1 - core], kv_r)
    halo_received(opposite == 0, opposite == NX - 1)

    power = HEAD ** (-0.5) * np.log2(np.e).item()
    to_scores = HEAD**0.5
    i_query = lax.broadcasted_iota(jnp.int32, (PAIR, 3 * PAIR), 0) % BLOCK + core * BLOCK
    i_key = lax.broadcasted_iota(jnp.int32, (PAIR, 3 * PAIR), 1) - PAIR
    near = jnp.abs(i_key - i_query) <= SIDE
    upper = lax.broadcasted_iota(jnp.int32, (PAIR, 1), 0) < BLOCK
    across = (((1,), (1,)), ((), ()))

    def attend(b, slot, heads=(0, 1)):
        key_at = i_key + (sp * NT * BLOCK + b * PAIR)
        valid = near & (key_at >= 0) & (key_at < TOKENS)
        for h in heads:
            q = query[b, pl.ds(2 * h, 2)].reshape(PAIR, HEAD)
            k_band = kv[pl.ds(b, 3), :, h].reshape(3 * PAIR, HEAD)
            v_band = kv[pl.ds(b, 3), :, 2 + h].reshape(3 * PAIR, HEAD)
            k_ctx = ckv[h, :, :, :, 0:HEAD].reshape(NSP * CTX_ROWS, HEAD)
            v_ctx = ckv[h, :, :, :, HEAD : 2 * HEAD].reshape(NSP * CTX_ROWS, HEAD)
            s_band = lax.dot_general(q, k_band, across, preferred_element_type=F32)
            s_band = jnp.where(valid, s_band, MASKED)
            s_ctx = lax.dot_general(q, k_ctx, across, preferred_element_type=F32)
            sinks = jnp.where(upper, sink[4 * x + 2 * h], sink[4 * x + 2 * h + 1]) * to_scores
            top = jnp.maximum(
                jnp.maximum(jnp.max(s_band, axis=-1, keepdims=True), jnp.max(s_ctx, axis=-1, keepdims=True)), sinks
            )
            e_band = jnp.exp2((s_band - top) * power)
            e_ctx = jnp.exp2((s_ctx - top) * power)
            total = (
                jnp.sum(e_band, axis=-1, keepdims=True)
                + jnp.sum(e_ctx, axis=-1, keepdims=True)
                + jnp.exp2((sinks - top) * power)
            )
            value = jnp.dot(e_band.astype(BF16), v_band, preferred_element_type=F32)
            value += jnp.dot(e_ctx.astype(BF16), v_ctx, preferred_element_type=F32)
            value = (value / total).astype(BF16)
            rows = slice(slot * BLOCK, (slot + 1) * BLOCK)
            for g in range(2):
                attended[h, rows, g * HEAD : (g + 1) * HEAD] = value[g * BLOCK : (g + 1) * BLOCK]

    def output(slot, slots, at, width):
        rows = slice(slot * BLOCK, (slot + slots) * BLOCK)
        columns = slice(at, at + width)
        result = jnp.dot(attended[0, rows, :], w_out[0, :, columns], preferred_element_type=F32)
        result += jnp.dot(attended[1, rows, :], w_out[1, :, columns], preferred_element_type=F32)
        result = result.astype(BF16)
        for s in range(slots):
            partial[slot + s, :, columns] = result[s * BLOCK : (s + 1) * BLOCK]

    attend(opposite, 3, (core,))
    received(ckv.at[1 - core], cc_r)
    attend(opposite, 3, (1 - core,))
    received(w_out.at[1 - core], wo_r)
    ring_s = one()
    left_r, right_r = pair()
    drained_at_end(partial.at[0:3], ring_s)
    for c in range(PIECES):
        output(3, 1, c * PIECE, PIECE)
        output(3, 1, HALF + c * PIECE, PIECE)
        lower = pl.ds(c * PIECE, PIECE)
        higher = pl.ds(HALF + c * PIECE, PIECE)
        send(partial.at[3, :, lower], from_left.at[:, lower], ring_s, o_r.at[0, c], to_right)
        send(partial.at[3, :, higher], from_right.at[:, lower], ring_s, o_r.at[1, c], to_left)
    halo_received(opposite != 0, opposite != NX - 1)
    attend(right, 1)
    attend(left, 2)
    for c in range(2 * PIECES):
        output(1, 2, c * PIECE, PIECE)
    low, high = pl.ds(0, HALF), pl.ds(HALF, HALF)
    send(partial.at[1, :, high], left_done.at[:, high], ring_s, left_r, to_right)
    send(partial.at[2, :, low], right_done.at[:, low], ring_s, right_r, to_left)
    for c in range(PIECES):
        lower = pl.ds(c * PIECE, PIECE)
        higher = pl.ds(HALF + c * PIECE, PIECE)
        received(from_left.at[:, lower], o_r.at[0, c])
        partial[1, :, lower] = (partial[1, :, lower].astype(F32) + from_left[:, lower].astype(F32)).astype(BF16)
        send(partial.at[1, :, lower], left_done.at[:, lower], ring_s, c_r.at[0, c], to_right)
        received(from_right.at[:, lower], o_r.at[1, c])
        partial[2, :, higher] = (partial[2, :, higher].astype(F32) + from_right[:, lower].astype(F32)).astype(BF16)
        send(partial.at[2, :, higher], right_done.at[:, higher], ring_s, c_r.at[1, c], to_left)
    attend(x, 0)
    for c in range(2 * PIECES):
        output(0, 1, c * PIECE, PIECE)
    received(tg_buf.at[0:7], tg_r)
    for t in range(NT):
        for c in range(4):
            at = t * 512 + c * 128
            mod_rows[4:5, at : at + 128] = tg_buf[t, c : c + 1, :]
    received(left_done.at[:, high], left_r)
    received(right_done.at[:, low], right_r)
    for c in range(PIECES):
        for half, done in enumerate((left_done, right_done)):
            at = pl.ds(half * HALF + c * PIECE, PIECE)
            received(done.at[:, at], c_r.at[half, c])
            projected = partial[0, :, at].astype(F32) + left_done[:, at].astype(F32) + right_done[:, at].astype(F32)
            out[:, at] = (x_raw[x, :, at].astype(F32) + mod_rows[4:5, at] * projected).astype(BF16)

    for copy in drains:
        copy.wait_send()


def shards(
    latent, context, cond, ctx_cond, w_shift, w_scale, w_gate, w_query, key_weight, value_weight, w_out, sink
):
    inverse = (THETA ** (-np.arange(HEAD // 4, dtype=np.float32) * np.float32(2.0) / np.float32(HEAD // 2))).astype(
        np.float32
    )
    inverse = jnp.asarray(np.tile(np.tile(inverse, 4)[None], (8, 1)))
    anywhere = pl.BlockSpec(memory_space=pl.ANY)
    inside = pl.BlockSpec(memory_space=pltpu.VMEM)
    dma = pltpu.SemaphoreType.DMA
    return pl.pallas_call(
        kernel,
        out_shape=pltpu.VMEM((BLOCK, WIDTH), BF16),
        in_specs=[anywhere] * 13,
        out_specs=inside,
        scratch_shapes=[
            pltpu.VMEM((2, NSP, 128), F32),
            pltpu.SMEM((16,), F32),
            pltpu.VMEM((8, 128), F32),
            pltpu.VMEM((NX, BLOCK, HEAD), F32),
            pltpu.VMEM((NX, BLOCK, HEAD), F32),
            pltpu.VMEM((NX, BLOCK, WIDTH), BF16),
            pltpu.VMEM((NX, BLOCK, 128), F32),
            pltpu.VMEM((NX, BLOCK, 128), F32),
            pltpu.VMEM((NX * BLOCK, WIDTH), BF16),
            pltpu.VMEM((2, WIDTH, 512), BF16),
            pltpu.VMEM((2, 256, WIDTH), BF16),
            pltpu.VMEM((3, 128, 512), BF16),
            pltpu.VMEM((CTX_ROWS, WIDTH), BF16),
            pltpu.VMEM((CTX_ROWS, WIDTH), BF16),
            pltpu.VMEM((NY, 24, 128), F32),
            pltpu.VMEM((NZ, 16, 128), F32),
            pltpu.VMEM((NT, 16, 128), F32),
            pltpu.VMEM((NZ, 8, 128), F32),
            pltpu.VMEM((NT, 8, 128), F32),
            pltpu.VMEM((8, WIDTH), F32),
            pltpu.VMEM((2, 2, NX * BLOCK, 256), BF16),
            pltpu.VMEM((NX, 4, BLOCK, HEAD), BF16),
            pltpu.VMEM((NX + 2, 2, 4, BLOCK, HEAD), BF16),
            pltpu.VMEM((2, NY, NZ, CTX_ROWS, 256), BF16),
            pltpu.VMEM((2, NX * BLOCK, 2 * HEAD), BF16),
            pltpu.VMEM((NX, BLOCK, WIDTH), BF16),
            pltpu.VMEM((BLOCK, HALF), BF16),
            pltpu.VMEM((BLOCK, HALF), BF16),
            pltpu.VMEM((BLOCK, WIDTH), BF16),
            pltpu.VMEM((BLOCK, WIDTH), BF16),
            dma((8,)), dma((6,)), dma((3,)), dma((4,)), dma((2, PIECES)), dma((2, PIECES)), dma((SINGLE,)),
        ],
        compiler_params=pltpu.CompilerParams(
            collective_id=0, has_side_effects=True, vmem_limit_bytes=60 * 1024 * 1024
        ),
    )(
        latent, context, cond.reshape(NSP, 128), ctx_cond.reshape(NSP, 128), w_shift, w_scale, w_gate,
        w_query, key_weight, value_weight, w_out, sink, inverse,
    )


def solution(mesh):
    in_specs = (
        P(("sp", "tp"), None), P("sp", None), P(), P(), P("sp", "tp"), P("sp", "tp"), P("sp", "tp"),
        P(None, "tp"), P(None, "tp"), P(None, "tp"), P("tp", None), P(),
    )
    out_specs = P(("sp", "tp"), None)
    return jax.shard_map(shards, mesh=mesh, in_specs=in_specs, out_specs=out_specs, check_vma=False)
```
